32 devices in a mesh: fs: 8 (over z, x), tp: 4 (over y, core).
Axes of the slice: x: 2, y: 2, z: 4, core: 2. Of those that a mesh axis runs over, the one named last changes fastest.
Arguments:
- stream: bfloat16 [4096, 2048], P('fs', 'tp'), may hold values from -6 to 6
- gain_mix: float32 [2048], replicated, may hold values from 0.1 to 1.9
- pool_weight: bfloat16 [4, 512, 512], P(None, 'fs', 'tp'), may hold values from -0.25 to 0.25
- pool_gain: float32 [2048], replicated, may hold values from 0.1 to 1.9
- gain_ffn: float32 [2048], replicated, may hold values from 0.1 to 1.9
- gate_weight: bfloat16 [2048, 5632], P('fs', 'tp'), may hold values from -0.125 to 0.125
- up_weight: bfloat16 [2048, 5632], P('fs', 'tp'), may hold values from -0.125 to 0.125
- gate_taps: float32 [3, 5632], replicated, may hold values from -2.5 to 2.5
- up_taps: float32 [3, 5632], replicated, may hold values from -2.5 to 2.5
- down_weight: bfloat16 [5632, 2048], P('tp', 'fs'), may hold values from -0.078125 to 0.078125
Outputs:
- layer_out: bfloat16 [4096, 2048], P('fs', 'tp')
The draws below stay inside these ranges and needn't reach their ends.
All inputs are finite; a program needn't handle non-finite values.
Results may differ from the reference program's by a relative error of at most 0.01.
Values may be sent and summed in bfloat16 or wider, within the bound.
A program may use at most 64 MiB of HBM per device.

```python
import jax
import jax.numpy as jnp
from jax import lax

D = 2048
G = 4
FF = 5632
TAPS = 3
LEN = 128
CG = 512
TOKENS = 4096


def level_of(own_key, dims, cuts, smallest, top_value):
    loudness, own = 1.0, jax.random.fold_in(own_key, 6)
    for axis_at, blocks in cuts:
        heights = jnp.exp(jax.random.uniform(jax.random.fold_in(own, axis_at), (blocks,), jnp.float32, smallest / len(cuts), top_value / len(cuts)))
        loudness = loudness * jnp.repeat(heights, dims[axis_at] // blocks).reshape([-1 if axis == axis_at else 1 for axis in range(len(dims))])
    return loudness


def scatter_about(own_key, shape, scale, limit, split=(), held_as=jnp.bfloat16):
    values = scale * jax.random.normal(own_key, shape, jnp.float32)
    if split:
        values = values * level_of(own_key, shape, split, -0.22, 0.18)
    return jnp.clip(values, -limit, limit).astype(held_as)


def setup_inputs(seed: int = 0) -> dict:
    streams_of = jax.random.split(jax.random.key(seed), 11)
    stream = scatter_about(streams_of[0], (TOKENS, D), 1.0, 6.0, ((0, 8), (1, 4)))
    gain_mix = jnp.clip(1.0 + 0.18 * jax.random.normal(streams_of[1], (D,), jnp.float32), 0.1, 1.9)
    pool_weight = scatter_about(streams_of[2], (G, CG, CG), CG ** -0.5, 0.25, ((1, 8), (2, 4)))
    pool_gain = jnp.clip(1.0 + 0.18 * jax.random.normal(streams_of[3], (D,), jnp.float32), 0.1, 1.9)
    gain_ffn = jnp.clip(1.0 + 0.18 * jax.random.normal(streams_of[4], (D,), jnp.float32), 0.1, 1.9)
    gate_weight = scatter_about(streams_of[5], (D, FF), D ** -0.5, 0.125, ((0, 8), (1, 4)))
    up_weight = scatter_about(streams_of[6], (D, FF), D ** -0.5, 0.125, ((0, 8), (1, 4)))
    gate_taps = scatter_about(streams_of[7], (TAPS, FF), 0.577, 2.5, (), jnp.float32)
    up_taps = scatter_about(streams_of[8], (TAPS, FF), 0.577, 2.5, (), jnp.float32)
    down_weight = scatter_about(streams_of[9], (FF, D), FF ** -0.5, 0.078125, ((0, 4), (1, 8)))
    return dict(stream=stream, gain_mix=gain_mix, pool_weight=pool_weight, pool_gain=pool_gain, gain_ffn=gain_ffn, gate_weight=gate_weight, up_weight=up_weight, gate_taps=gate_taps, up_taps=up_taps, down_weight=down_weight)


epsilon = 1e-06

def rms_norm(values, scales):
    return values * lax.rsqrt(lax.optimization_barrier(jnp.mean(values * values, axis=-1, keepdims=True)) + epsilon) * scales

def delayed(values, amount):
    return jnp.pad(values, ((0, 0), (amount, 0), (0, 0)))[:, :values.shape[1]]

def pool_less(values):
    channels = values.shape[2]
    group_id = jnp.arange(channels) % 4
    partials = [values]
    running = values
    for amount in (1, 2, 4, 8):
        running = running + delayed(running, amount)
        partials.append(running)
    picked = jnp.where(group_id == 0, partials[1], jnp.where(group_id == 1, partials[2], jnp.where(group_id == 2, partials[3], partials[4])))
    extent = jnp.where(group_id == 0, 2.0, jnp.where(group_id == 1, 4.0, jnp.where(group_id == 2, 8.0, 16.0)))
    position = jnp.arange(values.shape[1]).astype(jnp.float32)[:, None] + 1.0
    divisor = jnp.minimum(position, extent[None, :])
    return picked / divisor[None] - values

def causal_taps(values, kernel):
    reach = kernel.shape[0]
    length = values.shape[1]
    padded = jnp.pad(values, ((0, 0), (reach - 1, 0), (0, 0)))
    running = padded[:, 0:length] * kernel[0]
    for shift_by in range(1, reach):
        running = running + padded[:, shift_by:shift_by + length] * kernel[shift_by]
    return running

def reference(stream, gain_mix, pool_weight, pool_gain, gain_ffn, gate_weight, up_weight, gate_taps, up_taps, down_weight):
    tok_rows = stream.shape[0]
    seq_count = tok_rows // LEN
    normed = lax.optimization_barrier(rms_norm(stream.astype(jnp.float32), gain_mix).astype(jnp.bfloat16))
    pooled = pool_less(normed.astype(jnp.float32).reshape(seq_count, LEN, D)).astype(jnp.bfloat16)
    pooled = pooled.reshape(tok_rows, CG, G)
    mixer = jnp.einsum('tcg,gce->teg', pooled.astype(jnp.float32), pool_weight.astype(jnp.float32)).reshape(tok_rows, D) * pool_gain
    middle = lax.optimization_barrier((stream.astype(jnp.float32) + mixer).astype(jnp.bfloat16))
    normed_ffn = rms_norm(middle.astype(jnp.float32), gain_ffn).astype(jnp.bfloat16)
    gate_proj = lax.optimization_barrier(jnp.dot(normed_ffn, gate_weight, preferred_element_type=jnp.float32).astype(jnp.bfloat16))
    value_proj = lax.optimization_barrier(jnp.dot(normed_ffn, up_weight, preferred_element_type=jnp.float32).astype(jnp.bfloat16))
    gate_conv = causal_taps(gate_proj.astype(jnp.float32).reshape(seq_count, LEN, FF), gate_taps)
    value_conv = causal_taps(value_proj.astype(jnp.float32).reshape(seq_count, LEN, FF), up_taps)
    hidden = (jax.nn.silu(gate_conv) * value_conv).astype(jnp.bfloat16).reshape(tok_rows, FF)
    return jnp.dot(hidden, down_weight, preferred_element_type=jnp.float32).astype(jnp.bfloat16)
```

```python
import functools

import jax
import jax.numpy as jnp
from jax import lax
from jax.experimental import pallas as pl
from jax.experimental.pallas import tpu as pltpu
from jax.sharding import PartitionSpec as P

LEN = 128
GROUPS = 4
MESH = pl.DeviceIdType.MESH
epsilon = 1e-06

EARLY = (0, 1, 2, 3)
LATE = 4
CROSS = 5
FORE, BACK, SIDE = 0, 1, 2


def one_hot(rows, cols, hit):
    r = lax.broadcasted_iota(jnp.int32, (rows, cols), 0)
    c = lax.broadcasted_iota(jnp.int32, (rows, cols), 1)
    return jnp.where(hit(r, c), 1.0, 0.0).astype(jnp.bfloat16)


def delayed(values, amount):
    row = lax.broadcasted_iota(jnp.int32, values.shape, 0)
    return jnp.where(row < amount, 0.0, pltpu.roll(values, amount, 0))


def kernel(
    fs,
    tp,
    stream_ref,
    gain_mix_ref,
    pool_ref,
    pool_gain_ref,
    gain_ffn_ref,
    gate_ref,
    up_ref,
    gate_taps_ref,
    up_taps_ref,
    down_ref,
    out_ref,
    gate_all,
    up_all,
    down_all,
    pool_all,
    stream_all,
    middle_all,
    pooled,
    dense,
    normed_ffn,
    gate_sum,
    value_sum,
    hidden,
    part,
    theirs,
    total,
    w_send,
    w_recv,
    p_send,
    p_recv,
    a_send,
    a_recv,
    r_send,
    r_recv,
    own_sem,
):
    f = lax.axis_index("fs")
    t = lax.axis_index("tp")
    na = fs // 2
    a, b = f // 2, f % 2
    tokens, block = stream_ref.shape
    depth = gate_ref.shape[0]
    seqs = tokens // LEN
    cols = down_ref.shape[1]
    mate = t + 1 - 2 * (t % 2)

    barrier = pltpu.get_barrier_semaphore()
    for i in range(1, fs):
        pl.semaphore_signal(
            barrier, inc=1, device_id=(lax.rem(f + i, fs), t), device_id_type=MESH
        )
    for i in range(1, tp):
        pl.semaphore_signal(
            barrier, inc=1, device_id=(f, lax.rem(t + i, tp)), device_id_type=MESH
        )
    pl.semaphore_wait(barrier, fs + tp - 2)

    def act_copy(step, src, buf, owner, target):
        which = lax.rem(target - t + tp, tp)
        return pltpu.make_async_remote_copy(
            src_ref=src,
            dst_ref=buf.at[owner],
            send_sem=a_send.at[step, which, jnp.where(owner == t, 0, 1)],
            recv_sem=a_recv.at[step, owner],
            device_id=(f, target),
            device_id_type=MESH,
        )

    def act_start(step, src, buf):
        for i in range(2, tp, 2):
            act_copy(step, src, buf, t, lax.rem(t + i, tp)).start()
        act_copy(step, src, buf, t, mate).start()

    def act_relay(step, src, buf):
        for i in range(2, tp, 2):
            owner = lax.rem(t + i, tp)
            act_copy(step, buf.at[owner], buf, owner, mate).wait_recv()
            pltpu.make_async_remote_copy(
                src_ref=buf.at[owner],
                dst_ref=buf.at[owner],
                send_sem=a_send.at[step, i + 1, 1],
                recv_sem=a_recv.at[step, owner],
                device_id=(f, mate),
                device_id_type=MESH,
            ).start()
        for i in range(0, tp, 2):
            owner = lax.rem(mate + i, tp)
            act_copy(step, src, buf, owner, mate).wait_recv()

    def act_finish(step, src, buf):
        for i in range(2, tp, 2):
            act_copy(step, src, buf, t, lax.rem(t + i, tp)).wait_send()
            pltpu.make_async_remote_copy(
                src_ref=src,
                dst_ref=src,
                send_sem=a_send.at[step, i + 1, 1],
                recv_sem=a_recv.at[step, 0],
                device_id=(f, mate),
                device_id_type=MESH,
            ).wait_send()
        act_copy(step, src, buf, t, mate).wait_send()

    def pool_copy(target):
        return pltpu.make_async_remote_copy(
            src_ref=pool_ref,
            dst_ref=pool_all.at[f],
            send_sem=p_send.at[target],
            recv_sem=p_recv.at[f],
            device_id=(target, t),
            device_id_type=MESH,
        )

    act_start(0, stream_ref, stream_all)
    for i in range(1, fs):
        pool_copy(lax.rem(f + i, fs)).start()

    def slot(src, k):
        full = (gate_all, up_all, down_all)[k // 2]
        rows = full.shape[1] // 2
        return full.at[src, pl.ds((k % 2) * rows, rows)]

    def own(k):
        full = (gate_ref, up_ref, down_ref)[k // 2]
        rows = full.shape[0] // 2
        return full.at[pl.ds((k % 2) * rows, rows)]

    def piece(src, k, way, ref=None):
        target = (f + 2, f - 2, f + 1 - 2 * b)[way]
        return pltpu.make_async_remote_copy(
            src_ref=slot(src, k) if ref is None else ref,
            dst_ref=slot(src, k),
            send_sem=w_send.at[way, src, k],
            recv_sem=w_recv.at[src, k],
            device_id=(target, t),
            device_id_type=MESH,
        )

    def along(src, k, ref=None):
        @pl.when(a < na - 1)
        def _():
            piece(src, k, FORE, ref).start()

        @pl.when(a > 0)
        def _():
            piece(src, k, BACK, ref).start()

    pair = f + 1 - 2 * b
    piece(f, CROSS, SIDE, own(CROSS)).start()
    for k in EARLY:
        along(f, k, own(k))
        piece(f, k, SIDE, own(k)).start()
    locals_ = [
        pltpu.make_async_copy(stream_ref, stream_all.at[t], own_sem.at[0]),
        pltpu.make_async_copy(pool_ref, pool_all.at[f], own_sem.at[1]),
        pltpu.make_async_copy(gate_ref, gate_all.at[f], own_sem.at[2]),
        pltpu.make_async_copy(up_ref, up_all.at[f], own_sem.at[3]),
        pltpu.make_async_copy(down_ref, down_all.at[f], own_sem.at[4]),
    ]
    for copy in locals_:
        copy.start()

    def arrive(src, k, way):
        piece(src, k, way).wait_recv()
        if way == FORE:

            @pl.when(a < na - 1)
            def _():
                piece(src, k, FORE).start()

        else:

            @pl.when(a > 0)
            def _():
                piece(src, k, BACK).start()

    def events(d, ks):
        for k in ks:
            for way in (FORE, BACK):
                source = a - d if way == FORE else a + d

                @pl.when((source >= 0) & (source < na))
                def _():
                    src = source * 2 + b
                    arrive(src, k, way)
                    if k == CROSS:
                        arrive(source * 2 + 1 - b, k, way)
                    else:
                        piece(src, k, SIDE).start()

    for i in range(1, fs):
        src = lax.rem(f + i, fs)
        pltpu.make_async_remote_copy(
            src_ref=pool_ref,
            dst_ref=pool_all.at[src],
            send_sem=p_send.at[src],
            recv_sem=p_recv.at[src],
            device_id=(src, t),
            device_id_type=MESH,
        ).wait_recv()
    for copy in locals_:
        copy.wait()
    _, chans, outs = pool_ref.shape
    spread_rows = one_hot(
        GROUPS * chans,
        GROUPS * chans,
        lambda r, c: c == (r % GROUPS) * chans + r // GROUPS,
    )
    spread_cols = [
        one_hot(outs, GROUPS * outs, lambda r, c, g=g: c == r * GROUPS + g)
        for g in range(GROUPS)
    ]

    def densify(s, carry):
        wide = jnp.concatenate(
            [
                jnp.dot(
                    pool_all[s, g], spread_cols[g], preferred_element_type=jnp.float32
                )
                for g in range(GROUPS)
            ],
            axis=0,
        ).astype(jnp.bfloat16)
        rows = pl.ds(pl.multiple_of(s * GROUPS * chans, GROUPS * chans), GROUPS * chans)
        dense[rows, :] = jnp.dot(
            spread_rows, wide, preferred_element_type=jnp.float32
        ).astype(jnp.bfloat16)
        return carry

    lax.fori_loop(0, fs, densify, 0)

    act_relay(0, stream_ref, stream_all)

    def factor(buf, rows):
        square = jnp.zeros((LEN, 1), jnp.float32)
        for i in range(tp):
            v = buf[i, rows, :].astype(jnp.float32)
            square = square + jnp.sum(v * v, axis=-1, keepdims=True)
        return lax.rsqrt(square / (tp * block) + epsilon)

    def pool_seq(q, carry):
        rows = pl.ds(pl.multiple_of(q * LEN, LEN), LEN)
        scale = factor(stream_all, rows)
        lane = lax.broadcasted_iota(jnp.int32, (LEN, block), 1) % GROUPS
        row = lax.broadcasted_iota(jnp.int32, (LEN, block), 0)
        extent = jnp.where(lane == 0, 2, jnp.where(lane == 1, 4, jnp.where(lane == 2, 8, 16)))
        divisor = jnp.minimum(row + 1, extent).astype(jnp.float32)
        for i in range(tp):
            v = stream_all[i, rows, :].astype(jnp.float32)
            v = v * scale * gain_mix_ref[:, i * block : (i + 1) * block]
            v = v.astype(jnp.bfloat16).astype(jnp.float32)
            running = v + delayed(v, 1)
            picked = running
            for g, amount in ((1, 2), (2, 4), (3, 8)):
                running = running + delayed(running, amount)
                picked = jnp.where(lane >= g, running, picked)
            pooled[rows, i * block : (i + 1) * block] = (picked / divisor - v).astype(
                jnp.bfloat16
            )
        return carry

    lax.fori_loop(0, seqs, pool_seq, 0)

    def mix_seq(q, carry):
        rows = pl.ds(pl.multiple_of(q * LEN, LEN), LEN)
        mixed = jnp.dot(pooled[rows, :], dense[...], preferred_element_type=jnp.float32)
        total[rows, :] = (
            stream_ref[rows, :].astype(jnp.float32) + mixed * pool_gain_ref[...]
        ).astype(jnp.bfloat16)
        return carry

    lax.fori_loop(0, seqs, mix_seq, 0)

    act_start(1, total, middle_all)
    keep = pltpu.make_async_copy(total, middle_all.at[t], own_sem.at[0])
    keep.start()
    events(1, EARLY)
    gate_sum[...] = jnp.zeros_like(gate_sum)
    value_sum[...] = jnp.zeros_like(value_sum)
    keep.wait()
    act_relay(1, total, middle_all)

    def norm_seq(q, carry):
        rows = pl.ds(pl.multiple_of(q * LEN, LEN), LEN)
        scale = factor(middle_all, rows)
        for i in range(tp):
            span = slice(i * block, (i + 1) * block)
            v = middle_all[i, rows, :].astype(jnp.float32)
            normed_ffn[rows, span] = (v * scale * gain_ffn_ref[:, span]).astype(jnp.bfloat16)
        return carry

    lax.fori_loop(0, seqs, norm_seq, 0)

    def sources(d, take):
        def one(i, carry):
            far, up = i // 2, i % 2
            dist = d - far
            source = a + (2 * up - 1) * dist
            src = source * 2 + b + far - 2 * b * far
            exists = (source >= 0) & (source < na) & (dist >= 0) & (dist < na)

            @pl.when(exists & ((dist > 0) | (up == 0)))
            def _():
                take(src, source, far)

            return carry

        lax.fori_loop(0, 4, one, 0)

    half = tokens // 2

    def project(src, source, far):
        @pl.when(far == 1)
        def _():
            for k in EARLY:
                piece(src, k, SIDE).wait_recv()

        span = pl.ds(pl.multiple_of(src * depth, depth), depth)

        def chunk(m, carry):
            rows = pl.ds(pl.multiple_of(m * half, half), half)
            left = normed_ffn[rows, span]
            gate_sum[rows, :] += jnp.dot(
                left, gate_all[src], preferred_element_type=jnp.float32
            )
            value_sum[rows, :] += jnp.dot(
                left, up_all[src], preferred_element_type=jnp.float32
            )
            return carry

        lax.fori_loop(0, 2, chunk, 0)

    def late_start():
        along(f, LATE, own(LATE))
        piece(f, LATE, SIDE, own(LATE)).start()
        along(f, CROSS, own(CROSS))
        piece(pair, CROSS, SIDE).wait_recv()
        along(pair, CROSS)

    def early_round(d, carry):
        @pl.when((d >= 1) & (d <= na - 2))
        def _():
            events(d + 1, EARLY)

        @pl.when(d == na - 2)
        def _():
            late_start()

        @pl.when(d >= na - 1)
        def _():
            events(d - na + 2, (LATE, CROSS))

        sources(d, project)
        return carry

    lax.fori_loop(0, na + 1, early_round, 0)

    def gate_seq(q, carry):
        rows = pl.ds(pl.multiple_of(q * LEN, LEN), LEN)

        def conv(sums, taps):
            v = sums[rows, :].astype(jnp.bfloat16).astype(jnp.float32)
            reach = taps.shape[0]
            running = v * taps[reach - 1 : reach, :]
            for i in range(1, reach):
                running = running + delayed(v, i) * taps[reach - 1 - i : reach - i, :]
            return running

        gate = conv(gate_sum, gate_taps_ref)
        value = conv(value_sum, up_taps_ref)
        hidden[rows, :] = (gate / (1.0 + jnp.exp(-gate)) * value).astype(jnp.bfloat16)
        return carry

    lax.fori_loop(0, seqs, gate_seq, 0)

    def part_copy(src, source, col):
        return pltpu.make_async_remote_copy(
            src_ref=part.at[src],
            dst_ref=theirs.at[t, col],
            send_sem=r_send.at[src],
            recv_sem=r_recv.at[t, col],
            device_id=(f, source),
            device_id_type=MESH,
        )

    def finish(src, source, far):
        @pl.when(far == 1)
        def _():
            piece(src, LATE, SIDE).wait_recv()

        part[src] = jnp.dot(
            hidden[...], down_all[src], preferred_element_type=jnp.float32
        ).astype(jnp.bfloat16)

        @pl.when(source != t)
        def _():
            part_copy(src, source, src % 2).start()

    def late_round(d, carry):
        @pl.when((d >= 2) & (d + 1 < na))
        def _():
            events(d + 1, (LATE,))

        @pl.when((d >= 3) & (d < na))
        def _():
            events(d, (CROSS,))

        sources(d, finish)
        return carry

    lax.fori_loop(0, na + 1, late_round, 0)

    for col in range(2):
        for i in range(1, tp):
            peer = lax.rem(t + i, tp)
            pltpu.make_async_remote_copy(
                src_ref=part.at[0],
                dst_ref=theirs.at[peer, col],
                send_sem=r_send.at[0],
                recv_sem=r_recv.at[peer, col],
                device_id=(f, peer),
                device_id_type=MESH,
            ).wait_recv()
        summed = part[2 * t + col].astype(jnp.float32)
        for i in range(1, tp):
            summed = summed + theirs[lax.rem(t + i, tp), col].astype(jnp.float32)
        out_ref[:, col * cols : (col + 1) * cols] = summed.astype(out_ref.dtype)

    for i in range(1, fs):
        pool_copy(lax.rem(f + i, fs)).wait_send()
    act_finish(0, stream_ref, stream_all)
    act_finish(1, total, middle_all)

    def drain(s, carry):
        for k in range(6):
            line, col = s // 2, s % 2
            mine = (col == b) | (k == CROSS)

            @pl.when(mine & (a < na - 1) & (line <= a))
            def _():
                piece(s, k, FORE).wait_send()

            @pl.when(mine & (a > 0) & (line >= a))
            def _():
                piece(s, k, BACK).wait_send()

            @pl.when((s == f) if k == CROSS else (col == b))
            def _():
                piece(s, k, SIDE).wait_send()

        @pl.when(s // 2 != t)
        def _():
            part_copy(s, s // 2, s % 2).wait_send()

        return carry

    lax.fori_loop(0, fs, drain, 0)


def body(
    fs,
    tp,
    stream,
    gain_mix,
    pool_weight,
    pool_gain,
    gain_ffn,
    gate_weight,
    up_weight,
    gate_taps,
    up_taps,
    down_weight,
):
    tokens, block = stream.shape
    depth, width = gate_weight.shape
    cols = down_weight.shape[1]
    channels = gain_mix.shape[0]
    t = lax.axis_index("tp")

    def mine(values, size):
        return lax.dynamic_slice_in_dim(values, t * size, size, values.ndim - 1)

    bf16, f32 = jnp.bfloat16, jnp.float32
    dma = pltpu.SemaphoreType.DMA
    return pl.pallas_call(
        functools.partial(kernel, fs, tp),
        out_shape=jax.ShapeDtypeStruct((tokens, block), bf16),
        in_specs=[pl.BlockSpec(memory_space=pltpu.VMEM)] * 10,
        out_specs=pl.BlockSpec(memory_space=pltpu.VMEM),
        scratch_shapes=[
            pltpu.VMEM((fs, depth, width), bf16),
            pltpu.VMEM((fs, depth, width), bf16),
            pltpu.VMEM((fs, width, cols), bf16),
            pltpu.VMEM((fs,) + pool_weight.shape, bf16),
            pltpu.VMEM((tp, tokens, block), bf16),
            pltpu.VMEM((tp, tokens, block), bf16),
            pltpu.VMEM((tokens, channels), bf16),
            pltpu.VMEM((channels, block), bf16),
            pltpu.VMEM((tokens, channels), bf16),
            pltpu.VMEM((tokens, width), f32),
            pltpu.VMEM((tokens, width), f32),
            pltpu.VMEM((tokens, width), bf16),
            pltpu.VMEM((fs, tokens, cols), bf16),
            pltpu.VMEM((tp, 2, tokens, cols), bf16),
            pltpu.VMEM((tokens, block), bf16),
            dma((3, fs, 6)),
            dma((fs, 6)),
            dma((fs,)),
            dma((fs,)),
            dma((2, tp, 2)),
            dma((2, tp)),
            dma((fs,)),
            dma((tp, 2)),
            dma((5,)),
        ],
        compiler_params=pltpu.CompilerParams(
            collective_id=0, has_side_effects=True, vmem_limit_bytes=64 * 1024 * 1024 - 65536
        ),
    )(
        stream,
        gain_mix.reshape(1, channels),
        pool_weight,
        mine(pool_gain, block).reshape(1, block),
        gain_ffn.reshape(1, channels),
        gate_weight,
        up_weight,
        mine(gate_taps, width),
        mine(up_taps, width),
        down_weight,
    )


def solution(mesh):
    return jax.shard_map(
        functools.partial(body, mesh.shape["fs"], mesh.shape["tp"]),
        mesh=mesh,
        in_specs=(
            P("fs", "tp"),
            P(),
            P(None, "fs", "tp"),
            P(),
            P(),
            P("fs", "tp"),
            P("fs", "tp"),
            P(),
            P(),
            P("tp", "fs"),
        ),
        out_specs=P("fs", "tp"),
        check_vma=False,
    )
```

```python
import functools

import jax
import jax.numpy as jnp
from jax import lax
from jax.experimental import pallas as pl
from jax.experimental.pallas import tpu as pltpu
from jax.sharding import PartitionSpec as P

LEN = 128
GROUPS = 4
MESH = pl.DeviceIdType.MESH
epsilon = 1e-06

EARLY = (0, 1, 2, 3)
LATE = 4
CROSS = 5
FORE, BACK, SIDE = 0, 1, 2


def one_hot(rows, cols, hit):
    r = lax.broadcasted_iota(jnp.int32, (rows, cols), 0)
    c = lax.broadcasted_iota(jnp.int32, (rows, cols), 1)
    return jnp.where(hit(r, c), 1.0, 0.0).astype(jnp.bfloat16)


def delayed(values, amount):
    row = lax.broadcasted_iota(jnp.int32, values.shape, 0)
    return jnp.where(row < amount, 0.0, pltpu.roll(values, amount, 0))


def kernel(
    fs,
    tp,
    stream_ref,
    gain_mix_ref,
    pool_ref,
    pool_gain_ref,
    gain_ffn_ref,
    gate_ref,
    up_ref,
    gate_taps_ref,
    up_taps_ref,
    down_ref,
    out_ref,
    gate_all,
    up_all,
    down_all,
    pool_all,
    stream_all,
    middle_all,
    pooled,
    dense,
    normed_ffn,
    gate_sum,
    value_sum,
    hidden,
    part,
    theirs,
    total,
    w_send,
    w_recv,
    p_send,
    p_recv,
    a_send,
    a_recv,
    r_send,
    r_recv,
    own_sem,
):
    f = lax.axis_index("fs")
    t = lax.axis_index("tp")
    na = fs // 2
    a, b = f // 2, f % 2
    tokens, block = stream_ref.shape
    depth = gate_ref.shape[0]
    seqs = tokens // LEN
    cols = down_ref.shape[1]
    mate = t + 1 - 2 * (t % 2)

    barrier = pltpu.get_barrier_semaphore()
    for i in range(1, fs):
        pl.semaphore_signal(
            barrier, inc=1, device_id=(lax.rem(f + i, fs), t), device_id_type=MESH
        )
    for i in range(1, tp):
        pl.semaphore_signal(
            barrier, inc=1, device_id=(f, lax.rem(t + i, tp)), device_id_type=MESH
        )
    pl.semaphore_wait(barrier, fs + tp - 2)

    def act_copy(step, src, buf, owner, target):
        which = lax.rem(target - t + tp, tp)
        return pltpu.make_async_remote_copy(
            src_ref=src,
            dst_ref=buf.at[owner],
            send_sem=a_send.at[step, which, jnp.where(owner == t, 0, 1)],
            recv_sem=a_recv.at[step, owner],
            device_id=(f, target),
            device_id_type=MESH,
        )

    def act_start(step, src, buf):
        for i in range(2, tp, 2):
            act_copy(step, src, buf, t, lax.rem(t + i, tp)).start()
        act_copy(step, src, buf, t, mate).start()

    def act_relay(step, src, buf):
        for i in range(2, tp, 2):
            owner = lax.rem(t + i, tp)
            act_copy(step, buf.at[owner], buf, owner, mate).wait_recv()
            pltpu.make_async_remote_copy(
                src_ref=buf.at[owner],
                dst_ref=buf.at[owner],
                send_sem=a_send.at[step, i + 1, 1],
                recv_sem=a_recv.at[step, owner],
                device_id=(f, mate),
                device_id_type=MESH,
            ).start()
        for i in range(0, tp, 2):
            owner = lax.rem(mate + i, tp)
            act_copy(step, src, buf, owner, mate).wait_recv()

    def act_finish(step, src, buf):
        for i in range(2, tp, 2):
            act_copy(step, src, buf, t, lax.rem(t + i, tp)).wait_send()
            pltpu.make_async_remote_copy(
                src_ref=src,
                dst_ref=src,
                send_sem=a_send.at[step, i + 1, 1],
                recv_sem=a_recv.at[step, 0],
                device_id=(f, mate),
                device_id_type=MESH,
            ).wait_send()
        act_copy(step, src, buf, t, mate).wait_send()

    def pool_copy(target):
        return pltpu.make_async_remote_copy(
            src_ref=pool_ref,
            dst_ref=pool_all.at[f],
            send_sem=p_send.at[target],
            recv_sem=p_recv.at[f],
            device_id=(target, t),
            device_id_type=MESH,
        )

    act_start(0, stream_ref, stream_all)
    for i in range(1, fs):
        pool_copy(lax.rem(f + i, fs)).start()

    def slot(src, k):
        full = (gate_all, up_all, down_all)[k // 2]
        rows = full.shape[1] // 2
        return full.at[src, pl.ds((k % 2) * rows, rows)]

    def own(k):
        full = (gate_ref, up_ref, down_ref)[k // 2]
        rows = full.shape[0] // 2
        return full.at[pl.ds((k % 2) * rows, rows)]

    def piece(src, k, way, ref=None):
        target = (f + 2, f - 2, f + 1 - 2 * b)[way]
        return pltpu.make_async_remote_copy(
            src_ref=slot(src, k) if ref is None else ref,
            dst_ref=slot(src, k),
            send_sem=w_send.at[way, src, k],
            recv_sem=w_recv.at[src, k],
            device_id=(target, t),
            device_id_type=MESH,
        )

    def along(src, k, ref=None):
        @pl.when(a < na - 1)
        def _():
            piece(src, k, FORE, ref).start()

        @pl.when(a > 0)
        def _():
            piece(src, k, BACK, ref).start()

    pair = f + 1 - 2 * b
    piece(f, CROSS, SIDE, own(CROSS)).start()
    for k in EARLY:
        along(f, k, own(k))
        piece(f, k, SIDE, own(k)).start()
    locals_ = [
        pltpu.make_async_copy(stream_ref, stream_all.at[t], own_sem.at[0]),
        pltpu.make_async_copy(pool_ref, pool_all.at[f], own_sem.at[1]),
        pltpu.make_async_copy(gate_ref, gate_all.at[f], own_sem.at[2]),
        pltpu.make_async_copy(up_ref, up_all.at[f], own_sem.at[3]),
        pltpu.make_async_copy(down_ref, down_all.at[f], own_sem.at[4]),
    ]
    for copy in locals_:
        copy.start()

    def arrive(src, k, way):
        piece(src, k, way).wait_recv()
        if way == FORE:

            @pl.when(a < na - 1)
            def _():
                piece(src, k, FORE).start()

        else:

            @pl.when(a > 0)
            def _():
                piece(src, k, BACK).start()

    def events(d, ks):
        for k in ks:
            for way in (FORE, BACK):
                source = a - d if way == FORE else a + d

                @pl.when((source >= 0) & (source < na))
                def _():
                    src = source * 2 + b
                    arrive(src, k, way)
                    if k == CROSS:
                        arrive(source * 2 + 1 - b, k, way)
                    else:
                        piece(src, k, SIDE).start()

    for i in range(1, fs):
        src = lax.rem(f + i, fs)
        pltpu.make_async_remote_copy(
            src_ref=pool_ref,
            dst_ref=pool_all.at[src],
            send_sem=p_send.at[src],
            recv_sem=p_recv.at[src],
            device_id=(src, t),
            device_id_type=MESH,
        ).wait_recv()
    for copy in locals_:
        copy.wait()
    _, chans, outs = pool_ref.shape
    spread_rows = one_hot(
        GROUPS * chans,
        GROUPS * chans,
        lambda r, c: c == (r % GROUPS) * chans + r // GROUPS,
    )
    spread_cols = [
        one_hot(outs, GROUPS * outs, lambda r, c, g=g: c == r * GROUPS + g)
        for g in range(GROUPS)
    ]

    def densify(s, carry):
        wide = jnp.concatenate(
            [
                jnp.dot(
                    pool_all[s, g], spread_cols[g], preferred_element_type=jnp.float32
                )
                for g in range(GROUPS)
            ],
            axis=0,
        ).astype(jnp.bfloat16)
        rows = pl.ds(pl.multiple_of(s * GROUPS * chans, GROUPS * chans), GROUPS * chans)
        dense[rows, :] = jnp.dot(
            spread_rows, wide, preferred_element_type=jnp.float32
        ).astype(jnp.bfloat16)
        return carry

    lax.fori_loop(0, fs, densify, 0)

    act_relay(0, stream_ref, stream_all)

    def factor(buf, rows):
        square = jnp.zeros((LEN, 1), jnp.float32)
        for i in range(tp):
            v = buf[i, rows, :].astype(jnp.float32)
            square = square + jnp.sum(v * v, axis=-1, keepdims=True)
        return lax.rsqrt(square / (tp * block) + epsilon)

    def pool_seq(q, carry):
        rows = pl.ds(pl.multiple_of(q * LEN, LEN), LEN)
        scale = factor(stream_all, rows)
        lane = lax.broadcasted_iota(jnp.int32, (LEN, block), 1) % GROUPS
        row = lax.broadcasted_iota(jnp.int32, (LEN, block), 0)
        extent = jnp.where(lane == 0, 2, jnp.where(lane == 1, 4, jnp.where(lane == 2, 8, 16)))
        divisor = jnp.minimum(row + 1, extent).astype(jnp.float32)
        for i in range(tp):
            v = stream_all[i, rows, :].astype(jnp.float32)
            v = v * scale * gain_mix_ref[:, i * block : (i + 1) * block]
            v = v.astype(jnp.bfloat16).astype(jnp.float32)
            running = v + delayed(v, 1)
            picked = running
            for g, amount in ((1, 2), (2, 4), (3, 8)):
                running = running + delayed(running, amount)
                picked = jnp.where(lane >= g, running, picked)
            pooled[rows, i * block : (i + 1) * block] = (picked / divisor - v).astype(
                jnp.bfloat16
            )
        return carry

    lax.fori_loop(0, seqs, pool_seq, 0)

    def mix_seq(q, carry):
        rows = pl.ds(pl.multiple_of(q * LEN, LEN), LEN)
        mixed = jnp.dot(pooled[rows, :], dense[...], preferred_element_type=jnp.float32)
        total[rows, :] = (
            stream_ref[rows, :].astype(jnp.float32) + mixed * pool_gain_ref[...]
        ).astype(jnp.bfloat16)
        return carry

    lax.fori_loop(0, seqs, mix_seq, 0)

    act_start(1, total, middle_all)
    keep = pltpu.make_async_copy(total, middle_all.at[t], own_sem.at[0])
    keep.start()
    events(1, EARLY)
    gate_sum[...] = jnp.zeros_like(gate_sum)
    value_sum[...] = jnp.zeros_like(value_sum)
    keep.wait()
    act_relay(1, total, middle_all)

    def norm_seq(q, carry):
        rows = pl.ds(pl.multiple_of(q * LEN, LEN), LEN)
        scale = factor(middle_all, rows)
        for i in range(tp):
            span = slice(i * block, (i + 1) * block)
            v = middle_all[i, rows, :].astype(jnp.float32)
            normed_ffn[rows, span] = (v * scale * gain_ffn_ref[:, span]).astype(jnp.bfloat16)
        return carry

    lax.fori_loop(0, seqs, norm_seq, 0)

    def sources(d, take):
        def one(i, carry):
            far, up = i // 2, i % 2
            dist = d - far
            source = a + (2 * up - 1) * dist
            src = source * 2 + b + far - 2 * b * far
            exists = (source >= 0) & (source < na) & (dist >= 0) & (dist < na)

            @pl.when(exists & ((dist > 0) | (up == 0)))
            def _():
                take(src, source, far)

            return carry

        lax.fori_loop(0, 4, one, 0)

    half = tokens // 2

    def project(src, source, far):
        @pl.when(far == 1)
        def _():
            for k in EARLY:
                piece(src, k, SIDE).wait_recv()

        span = pl.ds(pl.multiple_of(src * depth, depth), depth)

        def chunk(m, carry):
            rows = pl.ds(pl.multiple_of(m * half, half), half)
            left = normed_ffn[rows, span]
            gate_sum[rows, :] += jnp.dot(
                left, gate_all[src], preferred_element_type=jnp.float32
            )
            value_sum[rows, :] += jnp.dot(
                left, up_all[src], preferred_element_type=jnp.float32
            )
            return carry

        lax.fori_loop(0, 2, chunk, 0)

    def late_start():
        along(f, LATE, own(LATE))
        piece(f, LATE, SIDE, own(LATE)).start()
        along(f, CROSS, own(CROSS))
        piece(pair, CROSS, SIDE).wait_recv()
        along(pair, CROSS)

    def early_round(d, carry):
        @pl.when((d >= 1) & (d <= na - 2))
        def _():
            events(d + 1, EARLY)

        @pl.when(d == na - 2)
        def _():
            late_start()

        @pl.when(d >= na - 1)
        def _():
            events(d - na + 2, (LATE, CROSS))

        sources(d, project)
        return carry

    lax.fori_loop(0, na + 1, early_round, 0)

    def gate_seq(q, carry):
        rows = pl.ds(pl.multiple_of(q * LEN, LEN), LEN)

        def conv(sums, taps):
            v = sums[rows, :].astype(jnp.bfloat16).astype(jnp.float32)
            reach = taps.shape[0]
            running = v * taps[reach - 1 : reach, :]
            for i in range(1, reach):
                running = running + delayed(v, i) * taps[reach - 1 - i : reach - i, :]
            return running

        gate = conv(gate_sum, gate_taps_ref)
        value = conv(value_sum, up_taps_ref)
        hidden[rows, :] = (gate / (1.0 + jnp.exp(-gate)) * value).astype(jnp.bfloat16)
        return carry

    lax.fori_loop(0, seqs, gate_seq, 0)

    def part_copy(src, source, col):
        return pltpu.make_async_remote_copy(
            src_ref=part.at[src],
            dst_ref=theirs.at[t, col],
            send_sem=r_send.at[src],
            recv_sem=r_recv.at[t, col],
            device_id=(f, source),
            device_id_type=MESH,
        )

    def finish(src, source, far):
        @pl.when(far == 1)
        def _():
            piece(src, LATE, SIDE).wait_recv()

        part[src] = jnp.dot(
            hidden[...], down_all[src], preferred_element_type=jnp.float32
        ).astype(jnp.bfloat16)

        @pl.when(source != t)
        def _():
            part_copy(src, source, src % 2).start()

    def late_round(d, carry):
        @pl.when((d >= 2) & (d + 1 < na))
        def _():
            events(d + 1, (LATE,))

        @pl.when((d >= 3) & (d < na))
        def _():
            events(d, (CROSS,))

        sources(d, finish)
        return carry

    lax.fori_loop(0, na + 1, late_round, 0)

    for col in range(2):
        for i in range(1, tp):
            peer = lax.rem(t + i, tp)
            pltpu.make_async_remote_copy(
                src_ref=part.at[0],
                dst_ref=theirs.at[peer, col],
                send_sem=r_send.at[0],
                recv_sem=r_recv.at[peer, col],
                device_id=(f, peer),
                device_id_type=MESH,
            ).wait_recv()
        summed = part[2 * t + col].astype(jnp.float32)
        for i in range(1, tp):
            summed = summed + theirs[lax.rem(t + i, tp), col].astype(jnp.float32)
        out_ref[:, col * cols : (col + 1) * cols] = summed.astype(out_ref.dtype)

    for i in range(1, fs):
        pool_copy(lax.rem(f + i, fs)).wait_send()
    act_finish(0, stream_ref, stream_all)
    act_finish(1, total, middle_all)

    def drain(s, carry):
        for k in range(6):
            line, col = s // 2, s % 2
            mine = (col == b) | (k == CROSS)

            @pl.when(mine & (a < na - 1) & (line <= a))
            def _():
                piece(s, k, FORE).wait_send()

            @pl.when(mine & (a > 0) & (line >= a))
            def _():
                piece(s, k, BACK).wait_send()

            @pl.when((s == f) if k == CROSS else (col == b))
            def _():
                piece(s, k, SIDE).wait_send()

        @pl.when(s // 2 != t)
        def _():
            part_copy(s, s // 2, s % 2).wait_send()

        return carry

    lax.fori_loop(0, fs, drain, 0)


MAIN, MATE, ACROSS = 0, 1, 2


def split_kernel(
    fs,
    tp,
    stream_ref,
    gain_mix_ref,
    pool_ref,
    pool_gain_ref,
    gain_ffn_ref,
    gate_ref,
    up_ref,
    gate_taps_ref,
    up_taps_ref,
    down_ref,
    out_ref,
    gate_all,
    up_all,
    down_all,
    pool_all,
    stream_all,
    middle_all,
    pooled,
    dense,
    normed_ffn,
    gate_sum,
    value_sum,
    hidden,
    part,
    mate_part,
    y_own,
    y_part,
    z_own,
    z_part,
    total,
    w_send,
    w_recv,
    p_send,
    p_recv,
    a_send,
    a_recv,
    b_sem,
    m_send,
    m_recv,
    y_sem,
    z_sem,
    own_sem,
):
    f = lax.axis_index("fs")
    t = lax.axis_index("tp")
    a, b = f // 2, f % 2
    tokens, block = stream_ref.shape
    depth, width = gate_ref.shape
    held = gate_all.shape[2]
    other = width - held
    seqs = tokens // LEN
    cols = down_ref.shape[1]
    mate = t + 1 - 2 * (t % 2)
    across_y = lax.rem(t + 2, tp)
    h = a // 2
    has_mid = t % 2 == h
    near = a + 1 - 2 * (a % 2)
    far_in, far_out = 2 - h, 3 * (1 - h)
    inner = (a == 1) | (a == 2)
    partner = lax.rem(f + fs // 2, fs)
    pair = f + 1 - 2 * b

    barrier = pltpu.get_barrier_semaphore()
    for i in range(1, fs):
        pl.semaphore_signal(
            barrier, inc=1, device_id=(lax.rem(f + i, fs), t), device_id_type=MESH
        )
    for i in range(1, tp):
        pl.semaphore_signal(
            barrier, inc=1, device_id=(f, lax.rem(t + i, tp)), device_id_type=MESH
        )
    pl.semaphore_wait(barrier, fs + tp - 2)

    def act_view(step):
        if step == 0:
            return lambda owner: stream_all.at[owner]
        return lambda owner: middle_all.at[owner, pl.ds((step - 1) * tokens, tokens)]

    def act_copy(step, src, owner, target, role):
        return pltpu.make_async_remote_copy(
            src_ref=src,
            dst_ref=act_view(step)(owner),
            send_sem=a_send.at[step, role],
            recv_sem=a_recv.at[step, owner],
            device_id=(f, target),
            device_id_type=MESH,
        )

    def act_start(step, src):
        act_copy(step, src, t, across_y, 0).start()
        act_copy(step, src, t, mate, 1).start()

    def act_relay(step):
        view = act_view(step)
        act_copy(step, view(across_y), across_y, mate, 2).wait_recv()
        act_copy(step, view(across_y), across_y, mate, 2).start()
        act_copy(step, view(mate), mate, mate, 2).wait_recv()
        diagonal = lax.rem(mate + 2, tp)
        act_copy(step, view(diagonal), diagonal, mate, 2).wait_recv()

    def act_finish(step):
        view = act_view(step)
        for role in range(3):
            act_copy(step, view(t), t, mate, role).wait_send()

    def pool_copy(target, owner):
        return pltpu.make_async_remote_copy(
            src_ref=pool_ref,
            dst_ref=pool_all.at[owner],
            send_sem=p_send.at[target],
            recv_sem=p_recv.at[owner],
            device_id=(target, t),
            device_id_type=MESH,
        )

    act_start(0, stream_ref)
    for i in range(1, fs):
        pool_copy(lax.rem(f + i, fs), f).start()

    def slot(src, k):
        full = (gate_all, up_all, down_all)[k % 3]
        span = pl.ds(0, other) if k < 3 else pl.ds(other, held - other)
        if k % 3 == 2:
            return full.at[src, span]
        return full.at[src, :, span]

    def own(q, k):
        full = (gate_ref, up_ref, down_ref)[k % 3]
        if k < 3:
            span = pl.ds(pl.multiple_of(q * held, 128), other)
        else:
            span = pl.ds(other, held - other)
        if k % 3 == 2:
            return full.at[span]
        return full.at[:, span]

    def piece(src, k, way, ref=None):
        target = (pair, near * 2 + b, far_in * 2 + b)[way]
        return pltpu.make_async_remote_copy(
            src_ref=slot(src, k) if ref is None else ref,
            dst_ref=slot(src, k),
            send_sem=w_send.at[way, src, k],
            recv_sem=w_recv.at[src, k],
            device_id=(target, t),
            device_id_type=MESH,
        )

    def guarded(k, do):
        if k < 3:
            do()
        else:
            pl.when(has_mid)(do)

    def own_start(k):
        if k < 3:
            piece(f, k, ACROSS, own(1 - h, k)).start()
        else:

            @pl.when(jnp.logical_not(has_mid))
            def _():
                piece(f, k, ACROSS, own(1 - h, k)).start()

        def rest():
            piece(f, k, MATE, own(h, k)).start()
            piece(f, k, MAIN, own(h, k)).start()

        guarded(k, rest)

    def events(source, ks, passed):
        src = source * 2 + b
        for k in ks:

            def one():
                piece(src, k, MAIN).wait_recv()
                if passed:

                    @pl.when(inner)
                    def _():
                        piece(src, k, MATE).start()

                piece(src, k, MAIN).start()

            guarded(k, one)

    def arrived(src, ks):
        for k in ks:
            guarded(k, lambda: piece(src, k, MAIN).wait_recv())

    early, late = (0, 3, 1, 4), (2, 5)
    for k in early:
        own_start(k)

    def local(k):
        return pltpu.make_async_copy(own(h, k), slot(f, k), own_sem.at[k])

    for k in range(6):
        guarded(k, lambda: local(k).start())
    keep_stream = pltpu.make_async_copy(stream_ref, stream_all.at[t], own_sem.at[6])
    keep_pool = pltpu.make_async_copy(pool_ref, pool_all.at[f], own_sem.at[7])
    keep_stream.start()
    keep_pool.start()

    @pl.when(jnp.logical_not(has_mid))
    def _():
        gate_all[:, :, other:] = jnp.zeros((fs, depth, held - other), jnp.bfloat16)
        up_all[:, :, other:] = jnp.zeros((fs, depth, held - other), jnp.bfloat16)
        down_all[:, other:, :] = jnp.zeros((fs, held - other, cols), jnp.bfloat16)

    for i in range(1, fs):
        src = lax.rem(f + i, fs)
        pool_copy(src, src).wait_recv()
    keep_pool.wait()
    _, chans, outs = pool_ref.shape
    spread_rows = one_hot(
        GROUPS * chans,
        GROUPS * chans,
        lambda r, c: c == (r % GROUPS) * chans + r // GROUPS,
    )
    spread_cols = [
        one_hot(outs, GROUPS * outs, lambda r, c, g=g: c == r * GROUPS + g)
        for g in range(GROUPS)
    ]

    def densify(s, carry):
        wide = jnp.concatenate(
            [
                jnp.dot(
                    pool_all[s, g], spread_cols[g], preferred_element_type=jnp.float32
                )
                for g in range(GROUPS)
            ],
            axis=0,
        ).astype(jnp.bfloat16)
        rows = pl.ds(pl.multiple_of(s * GROUPS * chans, GROUPS * chans), GROUPS * chans)
        dense[rows, :] = jnp.dot(
            spread_rows, wide, preferred_element_type=jnp.float32
        ).astype(jnp.bfloat16)
        return carry

    lax.fori_loop(0, fs, densify, 0)
    keep_stream.wait()
    act_relay(0)

    def factor(buf, rows):
        square = jnp.zeros((LEN, 1), jnp.float32)
        for i in range(tp):
            v = buf[i, rows, :].astype(jnp.float32)
            square = square + jnp.sum(v * v, axis=-1, keepdims=True)
        return lax.rsqrt(square / (tp * block) + epsilon)

    def pool_seq(q, carry):
        rows = pl.ds(pl.multiple_of(q * LEN, LEN), LEN)
        scale = factor(stream_all, rows)
        lane = lax.broadcasted_iota(jnp.int32, (LEN, block), 1) % GROUPS
        row = lax.broadcasted_iota(jnp.int32, (LEN, block), 0)
        extent = jnp.where(lane == 0, 2, jnp.where(lane == 1, 4, jnp.where(lane == 2, 8, 16)))
        divisor = jnp.minimum(row + 1, extent).astype(jnp.float32)
        for i in range(tp):
            v = stream_all[i, rows, :].astype(jnp.float32)
            v = v * scale * gain_mix_ref[:, i * block : (i + 1) * block]
            v = v.astype(jnp.bfloat16).astype(jnp.float32)
            running = v + delayed(v, 1)
            picked = running
            for g, amount in ((1, 2), (2, 4), (3, 8)):
                running = running + delayed(running, amount)
                picked = jnp.where(lane >= g, running, picked)
            pooled[rows, i * block : (i + 1) * block] = (picked / divisor - v).astype(
                jnp.bfloat16
            )
        mixed = jnp.dot(pooled[rows, :], dense[...], preferred_element_type=jnp.float32)
        total[rows, :] = (
            stream_ref[rows, :].astype(jnp.float32) + mixed * pool_gain_ref[...]
        ).astype(jnp.bfloat16)
        return carry

    lax.fori_loop(0, seqs, pool_seq, 0)

    to_partner = pltpu.make_async_remote_copy(
        src_ref=total,
        dst_ref=middle_all.at[t, pl.ds(tokens, tokens)],
        send_sem=b_sem.at[0],
        recv_sem=b_sem.at[1],
        device_id=(partner, t),
        device_id_type=MESH,
    )
    to_partner.start()
    act_start(1, total)
    keep = pltpu.make_async_copy(total, middle_all.at[t, pl.ds(0, tokens)], own_sem.at[8])
    keep.start()
    events(near, early, False)
    keep.wait()
    act_relay(1)

    def norm(first):
        def norm_seq(q, carry):
            rows = pl.ds(pl.multiple_of(first + q * LEN, LEN), LEN)
            scale = factor(middle_all, rows)
            for i in range(tp):
                span = slice(i * block, (i + 1) * block)
                v = middle_all[i, rows, :].astype(jnp.float32)
                normed_ffn[rows, span] = (v * scale * gain_ffn_ref[:, span]).astype(
                    jnp.bfloat16
                )
            return carry

        lax.fori_loop(0, seqs, norm_seq, 0)

    norm(0)
    events(far_in, early, True)
    to_partner.wait_recv()
    act_start(2, middle_all.at[t, pl.ds(tokens, tokens)])
    events(far_out, early, True)
    for k in late:
        own_start(k)
    for k in range(6):
        guarded(k, lambda: local(k).wait())
    act_relay(2)
    norm(tokens)
    arrived(pair, early)
    for source in (near, far_in, far_out):
        arrived(source * 2 + 1 - b, early)

    chunk = 2 * LEN

    def project(m, carry):
        rows = pl.ds(pl.multiple_of(m * chunk, chunk), chunk)
        left = normed_ffn[rows, :]
        for full, sums in ((gate_all, gate_sum), (up_all, value_sum)):
            sums[rows, :] = jnp.dot(
                left,
                full[...].reshape(fs * depth, held),
                preferred_element_type=jnp.float32,
            ).astype(jnp.bfloat16)
        return carry

    def gate_seq(q, carry):
        rows = pl.ds(pl.multiple_of(q * LEN, LEN), LEN)

        def conv(sums, taps_ref):
            taps = jnp.concatenate(
                [
                    taps_ref[:, pl.ds(pl.multiple_of(h * held, 128), other)],
                    taps_ref[:, other:held],
                ],
                axis=1,
            )
            v = sums[rows, :].astype(jnp.float32)
            reach = taps.shape[0]
            running = v * taps[reach - 1 : reach, :]
            for i in range(1, reach):
                running = running + delayed(v, i) * taps[reach - 1 - i : reach - i, :]
            return running

        gate = conv(gate_sum, gate_taps_ref)
        value = conv(value_sum, up_taps_ref)
        hidden[rows, :] = (gate / (1.0 + jnp.exp(-gate)) * value).astype(jnp.bfloat16)
        return carry

    chunks = tokens // chunk
    lax.fori_loop(0, chunks, project, 0)
    events(near, late, False)
    lax.fori_loop(chunks, 2 * chunks, project, 0)
    events(far_in, late, True)
    lax.fori_loop(0, 2 * seqs, gate_seq, 0)

    def source_of(i):
        j, far = i // 2, i % 2
        line = jnp.where(
            j == 0, a, jnp.where(j == 1, near, jnp.where(j == 2, far_in, far_out))
        )
        return line, line * 2 + b + far - 2 * b * far, far

    def mate_copy(s):
        return pltpu.make_async_remote_copy(
            src_ref=part.at[s],
            dst_ref=mate_part.at[s],
            send_sem=m_send.at[s],
            recv_sem=m_recv.at[s],
            device_id=(f, mate),
            device_id_type=MESH,
        )

    def y_copy(col):
        return pltpu.make_async_remote_copy(
            src_ref=y_own.at[col],
            dst_ref=y_part.at[col],
            send_sem=y_sem.at[0, col],
            recv_sem=y_sem.at[1, col],
            device_id=(f, across_y),
            device_id_type=MESH,
        )

    def z_copy(col):
        return pltpu.make_async_remote_copy(
            src_ref=z_own.at[col],
            dst_ref=z_part.at[col],
            send_sem=z_sem.at[0, col],
            recv_sem=z_sem.at[1, col],
            device_id=(partner, t),
            device_id_type=MESH,
        )

    steps = 2 * fs // 2

    def finish(i, carry):
        @pl.when(i == 5)
        def _():
            events(far_out, late, True)

        @pl.when(i < steps)
        def _():
            line, s, far = source_of(i)

            @pl.when(far == 1)
            def _():
                arrived(s, late)

            part[s] = jnp.dot(
                hidden[...], down_all[s], preferred_element_type=jnp.float32
            ).astype(jnp.bfloat16)

            @pl.when(line % 2 != t % 2)
            def _():
                mate_copy(s).start()

        @pl.when((i >= 1) & (i <= steps))
        def _():
            line, s, _ = source_of(i - 1)

            @pl.when(line % 2 == t % 2)
            def _():
                mate_copy(s).wait_recv()

                @pl.when(line != t)
                def _():
                    y_own[s % 2] = (
                        part[s].astype(jnp.float32) + mate_part[s].astype(jnp.float32)
                    ).astype(jnp.bfloat16)
                    y_copy(s % 2).start()

        @pl.when(i >= 2)
        def _():
            line, s, _ = source_of(i - 2)

            @pl.when(line == t)
            def _():
                col = s % 2
                y_copy(col).wait_recv()
                theirs = pl.ds(tokens, tokens)
                z_own[col] = (
                    part[s, theirs, :].astype(jnp.float32)
                    + mate_part[s, theirs, :].astype(jnp.float32)
                    + y_part[col, theirs, :].astype(jnp.float32)
                ).astype(jnp.bfloat16)
                z_copy(col).start()

        return carry

    lax.fori_loop(0, steps + 2, finish, 0)

    for col in range(2):
        z_copy(col).wait_recv()
        mine = pl.ds(0, tokens)
        s = 2 * t + col
        out_ref[:, col * cols : (col + 1) * cols] = (
            part[s, mine, :].astype(jnp.float32)
            + mate_part[s, mine, :].astype(jnp.float32)
            + y_part[col, mine, :].astype(jnp.float32)
            + z_part[col].astype(jnp.float32)
        ).astype(out_ref.dtype)

    for i in range(1, fs):
        pool_copy(lax.rem(f + i, fs), f).wait_send()
    for step in range(3):
        act_finish(step)
    to_partner.wait_send()
    for col in range(2):
        y_copy(col).wait_send()
        z_copy(col).wait_send()

    for k in range(6):
        if k < 3:
            piece(f, k, ACROSS, own(1 - h, k)).wait_send()
        else:

            @pl.when(jnp.logical_not(has_mid))
            def _():
                piece(f, k, ACROSS, own(1 - h, k)).wait_send()

        def rest():
            piece(f, k, MATE).wait_send()
            for line in (a, near, far_in, far_out):
                piece(line * 2 + b, k, MAIN).wait_send()

            @pl.when(inner)
            def _():
                for line in (far_in, far_out):
                    piece(line * 2 + b, k, MATE).wait_send()

        guarded(k, rest)

    def drain(s, carry):
        @pl.when((s // 2) % 2 != t % 2)
        def _():
            mate_copy(s).wait_send()

        return carry

    lax.fori_loop(0, fs, drain, 0)


def body(
    fs,
    tp,
    stream,
    gain_mix,
    pool_weight,
    pool_gain,
    gain_ffn,
    gate_weight,
    up_weight,
    gate_taps,
    up_taps,
    down_weight,
):
    tokens, block = stream.shape
    depth, width = gate_weight.shape
    cols = down_weight.shape[1]
    channels = gain_mix.shape[0]
    t = lax.axis_index("tp")

    def mine(values, size):
        return lax.dynamic_slice_in_dim(values, t * size, size, values.ndim - 1)

    bf16, f32 = jnp.bfloat16, jnp.float32
    dma = pltpu.SemaphoreType.DMA
    split = fs == 8 and tp == 4 and width % 256 == 128 and depth % 16 == 0
    if split:
        held = (width + 128) // 2
        run = split_kernel
        scratch = [
            pltpu.VMEM((fs, depth, held), bf16),
            pltpu.VMEM((fs, depth, held), bf16),
            pltpu.VMEM((fs, held, cols), bf16),
            pltpu.VMEM((fs,) + pool_weight.shape, bf16),
            pltpu.VMEM((tp, tokens, block), bf16),
            pltpu.VMEM((tp, 2 * tokens, block), bf16),
            pltpu.VMEM((tokens, channels), bf16),
            pltpu.VMEM((channels, block), bf16),
            pltpu.VMEM((2 * tokens, channels), bf16),
            pltpu.VMEM((2 * tokens, held), bf16),
            pltpu.VMEM((2 * tokens, held), bf16),
            pltpu.VMEM((2 * tokens, held), bf16),
            pltpu.VMEM((fs, 2 * tokens, cols), bf16),
            pltpu.VMEM((fs, 2 * tokens, cols), bf16),
            pltpu.VMEM((2, 2 * tokens, cols), bf16),
            pltpu.VMEM((2, 2 * tokens, cols), bf16),
            pltpu.VMEM((2, tokens, cols), bf16),
            pltpu.VMEM((2, tokens, cols), bf16),
            pltpu.VMEM((tokens, block), bf16),
            dma((3, fs, 6)),
            dma((fs, 6)),
            dma((fs,)),
            dma((fs,)),
            dma((3, 3)),
            dma((3, tp)),
            dma((2,)),
            dma((fs,)),
            dma((fs,)),
            dma((2, 2)),
            dma((2, 2)),
            dma((9,)),
        ]
    else:
        run = kernel
        scratch = [
            pltpu.VMEM((fs, depth, width), bf16),
            pltpu.VMEM((fs, depth, width), bf16),
            pltpu.VMEM((fs, width, cols), bf16),
            pltpu.VMEM((fs,) + pool_weight.shape, bf16),
            pltpu.VMEM((tp, tokens, block), bf16),
            pltpu.VMEM((tp, tokens, block), bf16),
            pltpu.VMEM((tokens, channels), bf16),
            pltpu.VMEM((channels, block), bf16),
            pltpu.VMEM((tokens, channels), bf16),
            pltpu.VMEM((tokens, width), f32),
            pltpu.VMEM((tokens, width), f32),
            pltpu.VMEM((tokens, width), bf16),
            pltpu.VMEM((fs, tokens, cols), bf16),
            pltpu.VMEM((tp, 2, tokens, cols), bf16),
            pltpu.VMEM((tokens, block), bf16),
            dma((3, fs, 6)),
            dma((fs, 6)),
            dma((fs,)),
            dma((fs,)),
            dma((2, tp, 2)),
            dma((2, tp)),
            dma((fs,)),
            dma((tp, 2)),
            dma((5,)),
        ]
    return pl.pallas_call(
        functools.partial(run, fs, tp),
        out_shape=jax.ShapeDtypeStruct((tokens, block), bf16),
        in_specs=[pl.BlockSpec(memory_space=pltpu.VMEM)] * 10,
        out_specs=pl.BlockSpec(memory_space=pltpu.VMEM),
        scratch_shapes=scratch,
        compiler_params=pltpu.CompilerParams(
            collective_id=0, has_side_effects=True, vmem_limit_bytes=64 * 1024 * 1024 - 65536
        ),
    )(
        stream,
        gain_mix.reshape(1, channels),
        pool_weight,
        mine(pool_gain, block).reshape(1, block),
        gain_ffn.reshape(1, channels),
        gate_weight,
        up_weight,
        mine(gate_taps, width),
        mine(up_taps, width),
        down_weight,
    )


def solution(mesh):
    return jax.shard_map(
        functools.partial(body, mesh.shape["fs"], mesh.shape["tp"]),
        mesh=mesh,
        in_specs=(
            P("fs", "tp"),
            P(),
            P(None, "fs", "tp"),
            P(),
            P(),
            P("fs", "tp"),
            P("fs", "tp"),
            P(),
            P(),
            P("tp", "fs"),
        ),
        out_specs=P("fs", "tp"),
        check_vma=False,
    )
```

```python
import functools

import jax
import jax.numpy as jnp
from jax import lax
from jax.experimental import pallas as pl
from jax.experimental.pallas import tpu as pltpu
from jax.sharding import PartitionSpec as P

LEN = 128
GROUPS = 4
MESH = pl.DeviceIdType.MESH
epsilon = 1e-06

EARLY = (0, 1, 2, 3)
LATE = 4
CROSS = 5
FORE, BACK, SIDE = 0, 1, 2


def one_hot(rows, cols, hit):
    r = lax.broadcasted_iota(jnp.int32, (rows, cols), 0)
    c = lax.broadcasted_iota(jnp.int32, (rows, cols), 1)
    return jnp.where(hit(r, c), 1.0, 0.0).astype(jnp.bfloat16)


def delayed(values, amount):
    row = lax.broadcasted_iota(jnp.int32, values.shape, 0)
    return jnp.where(row < amount, 0.0, pltpu.roll(values, amount, 0))


def kernel(
    fs,
    tp,
    stream_ref,
    gain_mix_ref,
    pool_ref,
    pool_gain_ref,
    gain_ffn_ref,
    gate_ref,
    up_ref,
    gate_taps_ref,
    up_taps_ref,
    down_ref,
    out_ref,
    gate_all,
    up_all,
    down_all,
    pool_all,
    stream_all,
    middle_all,
    pooled,
    dense,
    normed_ffn,
    gate_sum,
    value_sum,
    hidden,
    part,
    theirs,
    total,
    w_send,
    w_recv,
    p_send,
    p_recv,
    a_send,
    a_recv,
    r_send,
    r_recv,
    own_sem,
):
    f = lax.axis_index("fs")
    t = lax.axis_index("tp")
    na = fs // 2
    a, b = f // 2, f % 2
    tokens, block = stream_ref.shape
    depth = gate_ref.shape[0]
    seqs = tokens // LEN
    cols = down_ref.shape[1]
    mate = t + 1 - 2 * (t % 2)

    barrier = pltpu.get_barrier_semaphore()
    for i in range(1, fs):
        pl.semaphore_signal(
            barrier, inc=1, device_id=(lax.rem(f + i, fs), t), device_id_type=MESH
        )
    for i in range(1, tp):
        pl.semaphore_signal(
            barrier, inc=1, device_id=(f, lax.rem(t + i, tp)), device_id_type=MESH
        )
    pl.semaphore_wait(barrier, fs + tp - 2)

    def act_copy(step, src, buf, owner, target):
        which = lax.rem(target - t + tp, tp)
        return pltpu.make_async_remote_copy(
            src_ref=src,
            dst_ref=buf.at[owner],
            send_sem=a_send.at[step, which, jnp.where(owner == t, 0, 1)],
            recv_sem=a_recv.at[step, owner],
            device_id=(f, target),
            device_id_type=MESH,
        )

    def act_start(step, src, buf):
        for i in range(2, tp, 2):
            act_copy(step, src, buf, t, lax.rem(t + i, tp)).start()
        act_copy(step, src, buf, t, mate).start()

    def act_relay(step, src, buf):
        for i in range(2, tp, 2):
            owner = lax.rem(t + i, tp)
            act_copy(step, buf.at[owner], buf, owner, mate).wait_recv()
            pltpu.make_async_remote_copy(
                src_ref=buf.at[owner],
                dst_ref=buf.at[owner],
                send_sem=a_send.at[step, i + 1, 1],
                recv_sem=a_recv.at[step, owner],
                device_id=(f, mate),
                device_id_type=MESH,
            ).start()
        for i in range(0, tp, 2):
            owner = lax.rem(mate + i, tp)
            act_copy(step, src, buf, owner, mate).wait_recv()

    def act_finish(step, src, buf):
        for i in range(2, tp, 2):
            act_copy(step, src, buf, t, lax.rem(t + i, tp)).wait_send()
            pltpu.make_async_remote_copy(
                src_ref=src,
                dst_ref=src,
                send_sem=a_send.at[step, i + 1, 1],
                recv_sem=a_recv.at[step, 0],
                device_id=(f, mate),
                device_id_type=MESH,
            ).wait_send()
        act_copy(step, src, buf, t, mate).wait_send()

    def pool_copy(target):
        return pltpu.make_async_remote_copy(
            src_ref=pool_ref,
            dst_ref=pool_all.at[f],
            send_sem=p_send.at[target],
            recv_sem=p_recv.at[f],
            device_id=(target, t),
            device_id_type=MESH,
        )

    act_start(0, stream_ref, stream_all)
    for i in range(1, fs):
        pool_copy(lax.rem(f + i, fs)).start()

    def slot(src, k):
        full = (gate_all, up_all, down_all)[k // 2]
        rows = full.shape[1] // 2
        return full.at[src, pl.ds((k % 2) * rows, rows)]

    def own(k):
        full = (gate_ref, up_ref, down_ref)[k // 2]
        rows = full.shape[0] // 2
        return full.at[pl.ds((k % 2) * rows, rows)]

    def piece(src, k, way, ref=None):
        target = (f + 2, f - 2, f + 1 - 2 * b)[way]
        return pltpu.make_async_remote_copy(
            src_ref=slot(src, k) if ref is None else ref,
            dst_ref=slot(src, k),
            send_sem=w_send.at[way, src, k],
            recv_sem=w_recv.at[src, k],
            device_id=(target, t),
            device_id_type=MESH,
        )

    def along(src, k, ref=None):
        @pl.when(a < na - 1)
        def _():
            piece(src, k, FORE, ref).start()

        @pl.when(a > 0)
        def _():
            piece(src, k, BACK, ref).start()

    pair = f + 1 - 2 * b
    piece(f, CROSS, SIDE, own(CROSS)).start()
    for k in EARLY:
        along(f, k, own(k))
        piece(f, k, SIDE, own(k)).start()
    locals_ = [
        pltpu.make_async_copy(stream_ref, stream_all.at[t], own_sem.at[0]),
        pltpu.make_async_copy(pool_ref, pool_all.at[f], own_sem.at[1]),
        pltpu.make_async_copy(gate_ref, gate_all.at[f], own_sem.at[2]),
        pltpu.make_async_copy(up_ref, up_all.at[f], own_sem.at[3]),
        pltpu.make_async_copy(down_ref, down_all.at[f], own_sem.at[4]),
    ]
    for copy in locals_:
        copy.start()

    def arrive(src, k, way):
        piece(src, k, way).wait_recv()
        if way == FORE:

            @pl.when(a < na - 1)
            def _():
                piece(src, k, FORE).start()

        else:

            @pl.when(a > 0)
            def _():
                piece(src, k, BACK).start()

    def events(d, ks):
        for k in ks:
            for way in (FORE, BACK):
                source = a - d if way == FORE else a + d

                @pl.when((source >= 0) & (source < na))
                def _():
                    src = source * 2 + b
                    arrive(src, k, way)
                    if k == CROSS:
                        arrive(source * 2 + 1 - b, k, way)
                    else:
                        piece(src, k, SIDE).start()

    for i in range(1, fs):
        src = lax.rem(f + i, fs)
        pltpu.make_async_remote_copy(
            src_ref=pool_ref,
            dst_ref=pool_all.at[src],
            send_sem=p_send.at[src],
            recv_sem=p_recv.at[src],
            device_id=(src, t),
            device_id_type=MESH,
        ).wait_recv()
    for copy in locals_:
        copy.wait()
    _, chans, outs = pool_ref.shape
    spread_rows = one_hot(
        GROUPS * chans,
        GROUPS * chans,
        lambda r, c: c == (r % GROUPS) * chans + r // GROUPS,
    )
    spread_cols = [
        one_hot(outs, GROUPS * outs, lambda r, c, g=g: c == r * GROUPS + g)
        for g in range(GROUPS)
    ]

    def densify(s, carry):
        wide = jnp.concatenate(
            [
                jnp.dot(
                    pool_all[s, g], spread_cols[g], preferred_element_type=jnp.float32
                )
                for g in range(GROUPS)
            ],
            axis=0,
        ).astype(jnp.bfloat16)
        rows = pl.ds(pl.multiple_of(s * GROUPS * chans, GROUPS * chans), GROUPS * chans)
        dense[rows, :] = jnp.dot(
            spread_rows, wide, preferred_element_type=jnp.float32
        ).astype(jnp.bfloat16)
        return carry

    lax.fori_loop(0, fs, densify, 0)

    act_relay(0, stream_ref, stream_all)

    def factor(buf, rows):
        square = jnp.zeros((LEN, 1), jnp.float32)
        for i in range(tp):
            v = buf[i, rows, :].astype(jnp.float32)
            square = square + jnp.sum(v * v, axis=-1, keepdims=True)
        return lax.rsqrt(square / (tp * block) + epsilon)

    def pool_seq(q, carry):
        rows = pl.ds(pl.multiple_of(q * LEN, LEN), LEN)
        scale = factor(stream_all, rows)
        lane = lax.broadcasted_iota(jnp.int32, (LEN, block), 1) % GROUPS
        row = lax.broadcasted_iota(jnp.int32, (LEN, block), 0)
        extent = jnp.where(lane == 0, 2, jnp.where(lane == 1, 4, jnp.where(lane == 2, 8, 16)))
        divisor = jnp.minimum(row + 1, extent).astype(jnp.float32)
        for i in range(tp):
            v = stream_all[i, rows, :].astype(jnp.float32)
            v = v * scale * gain_mix_ref[:, i * block : (i + 1) * block]
            v = v.astype(jnp.bfloat16).astype(jnp.float32)
            running = v + delayed(v, 1)
            picked = running
            for g, amount in ((1, 2), (2, 4), (3, 8)):
                running = running + delayed(running, amount)
                picked = jnp.where(lane >= g, running, picked)
            pooled[rows, i * block : (i + 1) * block] = (picked / divisor - v).astype(
                jnp.bfloat16
            )
        return carry

    lax.fori_loop(0, seqs, pool_seq, 0)

    def mix_seq(q, carry):
        rows = pl.ds(pl.multiple_of(q * LEN, LEN), LEN)
        mixed = jnp.dot(pooled[rows, :], dense[...], preferred_element_type=jnp.float32)
        total[rows, :] = (
            stream_ref[rows, :].astype(jnp.float32) + mixed * pool_gain_ref[...]
        ).astype(jnp.bfloat16)
        return carry

    lax.fori_loop(0, seqs, mix_seq, 0)

    act_start(1, total, middle_all)
    keep = pltpu.make_async_copy(total, middle_all.at[t], own_sem.at[0])
    keep.start()
    events(1, EARLY)
    gate_sum[...] = jnp.zeros_like(gate_sum)
    value_sum[...] = jnp.zeros_like(value_sum)
    keep.wait()
    act_relay(1, total, middle_all)

    def norm_seq(q, carry):
        rows = pl.ds(pl.multiple_of(q * LEN, LEN), LEN)
        scale = factor(middle_all, rows)
        for i in range(tp):
            span = slice(i * block, (i + 1) * block)
            v = middle_all[i, rows, :].astype(jnp.float32)
            normed_ffn[rows, span] = (v * scale * gain_ffn_ref[:, span]).astype(jnp.bfloat16)
        return carry

    lax.fori_loop(0, seqs, norm_seq, 0)

    def sources(d, take):
        def one(i, carry):
            far, up = i // 2, i % 2
            dist = d - far
            source = a + (2 * up - 1) * dist
            src = source * 2 + b + far - 2 * b * far
            exists = (source >= 0) & (source < na) & (dist >= 0) & (dist < na)

            @pl.when(exists & ((dist > 0) | (up == 0)))
            def _():
                take(src, source, far)

            return carry

        lax.fori_loop(0, 4, one, 0)

    half = tokens // 2

    def project(src, source, far):
        @pl.when(far == 1)
        def _():
            for k in EARLY:
                piece(src, k, SIDE).wait_recv()

        span = pl.ds(pl.multiple_of(src * depth, depth), depth)

        def chunk(m, carry):
            rows = pl.ds(pl.multiple_of(m * half, half), half)
            left = normed_ffn[rows, span]
            gate_sum[rows, :] += jnp.dot(
                left, gate_all[src], preferred_element_type=jnp.float32
            )
            value_sum[rows, :] += jnp.dot(
                left, up_all[src], preferred_element_type=jnp.float32
            )
            return carry

        lax.fori_loop(0, 2, chunk, 0)

    def late_start():
        along(f, LATE, own(LATE))
        piece(f, LATE, SIDE, own(LATE)).start()
        along(f, CROSS, own(CROSS))
        piece(pair, CROSS, SIDE).wait_recv()
        along(pair, CROSS)

    def early_round(d, carry):
        @pl.when((d >= 1) & (d <= na - 2))
        def _():
            events(d + 1, EARLY)

        @pl.when(d == na - 2)
        def _():
            late_start()

        @pl.when(d >= na - 1)
        def _():
            events(d - na + 2, (LATE, CROSS))

        sources(d, project)
        return carry

    lax.fori_loop(0, na + 1, early_round, 0)

    def gate_seq(q, carry):
        rows = pl.ds(pl.multiple_of(q * LEN, LEN), LEN)

        def conv(sums, taps):
            v = sums[rows, :].astype(jnp.bfloat16).astype(jnp.float32)
            reach = taps.shape[0]
            running = v * taps[reach - 1 : reach, :]
            for i in range(1, reach):
                running = running + delayed(v, i) * taps[reach - 1 - i : reach - i, :]
            return running

        gate = conv(gate_sum, gate_taps_ref)
        value = conv(value_sum, up_taps_ref)
        hidden[rows, :] = (gate / (1.0 + jnp.exp(-gate)) * value).astype(jnp.bfloat16)
        return carry

    lax.fori_loop(0, seqs, gate_seq, 0)

    def part_copy(src, source, col):
        return pltpu.make_async_remote_copy(
            src_ref=part.at[src],
            dst_ref=theirs.at[t, col],
            send_sem=r_send.at[src],
            recv_sem=r_recv.at[t, col],
            device_id=(f, source),
            device_id_type=MESH,
        )

    def finish(src, source, far):
        @pl.when(far == 1)
        def _():
            piece(src, LATE, SIDE).wait_recv()

        part[src] = jnp.dot(
            hidden[...], down_all[src], preferred_element_type=jnp.float32
        ).astype(jnp.bfloat16)

        @pl.when(source != t)
        def _():
            part_copy(src, source, src % 2).start()

    def late_round(d, carry):
        @pl.when((d >= 2) & (d + 1 < na))
        def _():
            events(d + 1, (LATE,))

        @pl.when((d >= 3) & (d < na))
        def _():
            events(d, (CROSS,))

        sources(d, finish)
        return carry

    lax.fori_loop(0, na + 1, late_round, 0)

    for col in range(2):
        for i in range(1, tp):
            peer = lax.rem(t + i, tp)
            pltpu.make_async_remote_copy(
                src_ref=part.at[0],
                dst_ref=theirs.at[peer, col],
                send_sem=r_send.at[0],
                recv_sem=r_recv.at[peer, col],
                device_id=(f, peer),
                device_id_type=MESH,
            ).wait_recv()
        summed = part[2 * t + col].astype(jnp.float32)
        for i in range(1, tp):
            summed = summed + theirs[lax.rem(t + i, tp), col].astype(jnp.float32)
        out_ref[:, col * cols : (col + 1) * cols] = summed.astype(out_ref.dtype)

    for i in range(1, fs):
        pool_copy(lax.rem(f + i, fs)).wait_send()
    act_finish(0, stream_ref, stream_all)
    act_finish(1, total, middle_all)

    def drain(s, carry):
        for k in range(6):
            line, col = s // 2, s % 2
            mine = (col == b) | (k == CROSS)

            @pl.when(mine & (a < na - 1) & (line <= a))
            def _():
                piece(s, k, FORE).wait_send()

            @pl.when(mine & (a > 0) & (line >= a))
            def _():
                piece(s, k, BACK).wait_send()

            @pl.when((s == f) if k == CROSS else (col == b))
            def _():
                piece(s, k, SIDE).wait_send()

        @pl.when(s // 2 != t)
        def _():
            part_copy(s, s // 2, s % 2).wait_send()

        return carry

    lax.fori_loop(0, fs, drain, 0)


MAIN, MATE, ACROSS = 0, 1, 2


def split_kernel(
    fs,
    tp,
    stream_ref,
    gain_mix_ref,
    pool_ref,
    pool_gain_ref,
    gain_ffn_ref,
    gate_ref,
    up_ref,
    gate_taps_ref,
    up_taps_ref,
    down_ref,
    out_ref,
    gate_all,
    up_all,
    down_all,
    pool_all,
    stream_all,
    middle_all,
    pooled,
    dense,
    normed_ffn,
    gate_sum,
    value_sum,
    hidden,
    part,
    mate_part,
    y_own,
    y_part,
    z_own,
    z_part,
    total,
    w_send,
    w_recv,
    p_send,
    p_recv,
    a_send,
    a_recv,
    b_sem,
    m_send,
    m_recv,
    y_sem,
    z_sem,
    own_sem,
):
    f = lax.axis_index("fs")
    t = lax.axis_index("tp")
    a, b = f // 2, f % 2
    tokens, block = stream_ref.shape
    depth, width = gate_ref.shape
    held = gate_all.shape[2]
    other = width - held
    seqs = tokens // LEN
    cols = down_ref.shape[1]
    mate = t + 1 - 2 * (t % 2)
    across_y = lax.rem(t + 2, tp)
    h = a // 2
    has_mid = t % 2 == h
    near = a + 1 - 2 * (a % 2)
    far_in, far_out = 2 - h, 3 * (1 - h)
    inner = (a == 1) | (a == 2)
    partner = lax.rem(f + fs // 2, fs)
    pair = f + 1 - 2 * b

    barrier = pltpu.get_barrier_semaphore()
    for i in range(1, fs):
        pl.semaphore_signal(
            barrier, inc=1, device_id=(lax.rem(f + i, fs), t), device_id_type=MESH
        )
    for i in range(1, tp):
        pl.semaphore_signal(
            barrier, inc=1, device_id=(f, lax.rem(t + i, tp)), device_id_type=MESH
        )
    pl.semaphore_wait(barrier, fs + tp - 2)

    def act_view(step):
        buf = stream_all if step < 2 else middle_all
        return lambda owner: buf.at[owner, pl.ds((step % 2) * tokens, tokens)]

    def act_copy(step, src, owner, target, role):
        return pltpu.make_async_remote_copy(
            src_ref=src,
            dst_ref=act_view(step)(owner),
            send_sem=a_send.at[step, role],
            recv_sem=a_recv.at[step, owner],
            device_id=(f, target),
            device_id_type=MESH,
        )

    def act_start(step, src):
        act_copy(step, src, t, across_y, 0).start()
        act_copy(step, src, t, mate, 1).start()

    def act_relay(step):
        view = act_view(step)
        act_copy(step, view(across_y), across_y, mate, 2).wait_recv()
        act_copy(step, view(across_y), across_y, mate, 2).start()
        act_copy(step, view(mate), mate, mate, 2).wait_recv()
        diagonal = lax.rem(mate + 2, tp)
        act_copy(step, view(diagonal), diagonal, mate, 2).wait_recv()

    def act_finish(step):
        view = act_view(step)
        for role in range(3):
            act_copy(step, view(t), t, mate, role).wait_send()

    def pool_copy(target, owner):
        return pltpu.make_async_remote_copy(
            src_ref=pool_ref,
            dst_ref=pool_all.at[owner],
            send_sem=p_send.at[target],
            recv_sem=p_recv.at[owner],
            device_id=(target, t),
            device_id_type=MESH,
        )

    to_partner = pltpu.make_async_remote_copy(
        src_ref=stream_ref,
        dst_ref=stream_all.at[t, pl.ds(tokens, tokens)],
        send_sem=b_sem.at[0],
        recv_sem=b_sem.at[1],
        device_id=(partner, t),
        device_id_type=MESH,
    )

    def pool_pass(owner, ref):
        return pltpu.make_async_remote_copy(
            src_ref=ref,
            dst_ref=pool_all.at[owner],
            send_sem=p_send.at[owner // 2 * 2 + 1 - b],
            recv_sem=p_recv.at[owner],
            device_id=(pair, t),
            device_id_type=MESH,
        )

    act_start(0, stream_ref)
    for i in range(2, fs, 2):
        pool_copy(lax.rem(f + i, fs), f).start()
    pool_pass(f, pool_ref).start()
    to_partner.start()

    def slot(src, k):
        full = (gate_all, up_all, down_all)[k % 3]
        span = pl.ds(0, other) if k < 3 else pl.ds(other, held - other)
        if k % 3 == 2:
            return full.at[src, span]
        return full.at[src, :, span]

    def own(q, k):
        full = (gate_ref, up_ref, down_ref)[k % 3]
        if k < 3:
            span = pl.ds(pl.multiple_of(q * held, 128), other)
        else:
            span = pl.ds(other, held - other)
        if k % 3 == 2:
            return full.at[span]
        return full.at[:, span]

    def piece(src, k, way, ref=None):
        target = (pair, near * 2 + b, far_in * 2 + b)[way]
        return pltpu.make_async_remote_copy(
            src_ref=slot(src, k) if ref is None else ref,
            dst_ref=slot(src, k),
            send_sem=w_send.at[way, src, k],
            recv_sem=w_recv.at[src, k],
            device_id=(target, t),
            device_id_type=MESH,
        )

    def guarded(k, do):
        if k < 3:
            do()
        else:
            pl.when(has_mid)(do)

    def own_across(k):
        if k < 3:
            piece(f, k, ACROSS, own(1 - h, k)).start()
        else:

            @pl.when(jnp.logical_not(has_mid))
            def _():
                piece(f, k, ACROSS, own(1 - h, k)).start()

    def own_near(k):
        def rest():
            piece(f, k, MATE, own(h, k)).start()
            piece(f, k, MAIN, own(h, k)).start()

        guarded(k, rest)

    def events(source, ks, passed):
        src = source * 2 + b
        for k in ks:

            def one():
                piece(src, k, MAIN).wait_recv()
                if passed:

                    @pl.when(inner)
                    def _():
                        piece(src, k, MATE).start()

                piece(src, k, MAIN).start()

            guarded(k, one)

    def arrived(src, ks):
        for k in ks:
            guarded(k, lambda: piece(src, k, MAIN).wait_recv())

    early, late = (0, 3, 1, 4), (2, 5)
    for k in early:
        own_across(k)
        own_near(k)
    for k in late:
        own_across(k)

    def local(k):
        return pltpu.make_async_copy(own(h, k), slot(f, k), own_sem.at[k])

    for k in range(6):
        guarded(k, lambda: local(k).start())
    keep_stream = pltpu.make_async_copy(
        stream_ref, stream_all.at[t, pl.ds(0, tokens)], own_sem.at[6]
    )
    keep_pool = pltpu.make_async_copy(pool_ref, pool_all.at[f], own_sem.at[7])
    keep_stream.start()
    keep_pool.start()

    @pl.when(jnp.logical_not(has_mid))
    def _():
        gate_all[:, :, other:] = jnp.zeros((fs, depth, held - other), jnp.bfloat16)
        up_all[:, :, other:] = jnp.zeros((fs, depth, held - other), jnp.bfloat16)
        down_all[:, other:, :] = jnp.zeros((fs, held - other, cols), jnp.bfloat16)

    for i in range(2, fs, 2):
        src = lax.rem(f + i, fs)
        pool_copy(src, src).wait_recv()
        pool_pass(src, pool_all.at[src]).start()
    for i in range(0, fs, 2):
        src = lax.rem(pair + i, fs)
        pool_copy(src, src).wait_recv()
    keep_pool.wait()
    _, chans, outs = pool_ref.shape
    spread_rows = one_hot(
        GROUPS * chans,
        GROUPS * chans,
        lambda r, c: c == (r % GROUPS) * chans + r // GROUPS,
    )
    spread_cols = [
        one_hot(outs, GROUPS * outs, lambda r, c, g=g: c == r * GROUPS + g)
        for g in range(GROUPS)
    ]

    def densify(s, carry):
        wide = jnp.concatenate(
            [
                jnp.dot(
                    pool_all[s, g], spread_cols[g], preferred_element_type=jnp.float32
                )
                for g in range(GROUPS)
            ],
            axis=0,
        ).astype(jnp.bfloat16)
        rows = pl.ds(pl.multiple_of(s * GROUPS * chans, GROUPS * chans), GROUPS * chans)
        dense[rows, :] = jnp.dot(
            spread_rows, wide, preferred_element_type=jnp.float32
        ).astype(jnp.bfloat16)
        return carry

    lax.fori_loop(0, fs, densify, 0)
    keep_stream.wait()
    act_relay(0)

    def factor(buf, rows):
        square = jnp.zeros((LEN, 1), jnp.float32)
        for i in range(tp):
            v = buf[i, rows, :].astype(jnp.float32)
            square = square + jnp.sum(v * v, axis=-1, keepdims=True)
        return lax.rsqrt(square / (tp * block) + epsilon)

    def pool_seq(q, carry):
        rows = pl.ds(pl.multiple_of(q * LEN, LEN), LEN)
        scale = factor(stream_all, rows)
        lane = lax.broadcasted_iota(jnp.int32, (LEN, block), 1) % GROUPS
        row = lax.broadcasted_iota(jnp.int32, (LEN, block), 0)
        extent = jnp.where(lane == 0, 2, jnp.where(lane == 1, 4, jnp.where(lane == 2, 8, 16)))
        divisor = jnp.minimum(row + 1, extent).astype(jnp.float32)
        for i in range(tp):
            v = stream_all[i, rows, :].astype(jnp.float32)
            v = v * scale * gain_mix_ref[:, i * block : (i + 1) * block]
            v = v.astype(jnp.bfloat16).astype(jnp.float32)
            running = v + delayed(v, 1)
            picked = running
            for g, amount in ((1, 2), (2, 4), (3, 8)):
                running = running + delayed(running, amount)
                picked = jnp.where(lane >= g, running, picked)
            pooled[rows, i * block : (i + 1) * block] = (picked / divisor - v).astype(
                jnp.bfloat16
            )
        mixed = jnp.dot(pooled[rows, :], dense[...], preferred_element_type=jnp.float32)
        total[rows, :] = (
            stream_all[t, rows, :].astype(jnp.float32)
            + mixed * pool_gain_ref[:, pl.ds(pl.multiple_of(t * block, 128), block)]
        ).astype(jnp.bfloat16)
        return carry

    lax.fori_loop(0, seqs, pool_seq, 0)
    ours, theirs = pl.ds(0, tokens), pl.ds(tokens, tokens)
    act_start(2, total.at[ours])
    keep = [
        pltpu.make_async_copy(total.at[span], middle_all.at[t, span], own_sem.at[8 + i])
        for i, span in enumerate((ours, theirs))
    ]
    keep[0].start()
    to_partner.wait_recv()
    act_start(1, stream_all.at[t, theirs])
    events(near, early, False)
    act_relay(1)
    lax.fori_loop(seqs, 2 * seqs, pool_seq, 0)
    act_start(3, total.at[theirs])
    keep[1].start()
    keep[0].wait()
    act_relay(2)

    def norm(first):
        def norm_seq(q, carry):
            rows = pl.ds(pl.multiple_of(first + q * LEN, LEN), LEN)
            scale = factor(middle_all, rows)
            for i in range(tp):
                span = slice(i * block, (i + 1) * block)
                v = middle_all[i, rows, :].astype(jnp.float32)
                normed_ffn[rows, span] = (v * scale * gain_ffn_ref[:, span]).astype(
                    jnp.bfloat16
                )
            return carry

        lax.fori_loop(0, seqs, norm_seq, 0)

    events(far_in, early, True)
    for k in late:
        own_near(k)
    norm(0)
    keep[1].wait()
    act_relay(3)
    norm(tokens)
    events(far_out, early, True)
    for k in range(6):
        guarded(k, lambda: local(k).wait())
    arrived(pair, early)
    for source in (near, far_in, far_out):
        arrived(source * 2 + 1 - b, early)

    chunk = 2 * LEN

    def project(m, carry):
        rows = pl.ds(pl.multiple_of(m * chunk, chunk), chunk)
        left = normed_ffn[rows, :]
        for full, sums in ((gate_all, gate_sum), (up_all, value_sum)):
            sums[rows, :] = jnp.dot(
                left,
                full[...].reshape(fs * depth, held),
                preferred_element_type=jnp.float32,
            ).astype(jnp.bfloat16)
        return carry

    def gate_seq(q, carry):
        rows = pl.ds(pl.multiple_of(q * LEN, LEN), LEN)

        def conv(sums, taps_ref):
            taps = jnp.concatenate(
                [
                    taps_ref[:, pl.ds(pl.multiple_of(t * width + h * held, 128), other)],
                    taps_ref[:, pl.ds(pl.multiple_of(t * width + other, 128), held - other)],
                ],
                axis=1,
            )
            v = sums[rows, :].astype(jnp.float32)
            reach = taps.shape[0]
            running = v * taps[reach - 1 : reach, :]
            for i in range(1, reach):
                running = running + delayed(v, i) * taps[reach - 1 - i : reach - i, :]
            return running

        gate = conv(gate_sum, gate_taps_ref)
        value = conv(value_sum, up_taps_ref)
        hidden[rows, :] = (gate / (1.0 + jnp.exp(-gate)) * value).astype(jnp.bfloat16)
        return carry

    chunks = tokens // chunk
    lax.fori_loop(0, chunks, project, 0)
    events(near, late, False)
    lax.fori_loop(chunks, 2 * chunks, project, 0)
    events(far_in, late, True)
    lax.fori_loop(0, 2 * seqs, gate_seq, 0)

    def source_of(i):
        far = jnp.where((i == 2) | (i == 4) | (i == 5) | (i == 7), 1, 0)
        line = jnp.where(
            (i == 0) | (i == 2),
            a,
            jnp.where((i == 3) | (i == 4), near, jnp.where(i >= 6, far_out, far_in)),
        )
        return line, line * 2 + b + far - 2 * b * far, far

    def mate_copy(s):
        return pltpu.make_async_remote_copy(
            src_ref=part.at[s],
            dst_ref=mate_part.at[s],
            send_sem=m_send.at[s],
            recv_sem=m_recv.at[s],
            device_id=(f, mate),
            device_id_type=MESH,
        )

    def y_copy(col):
        return pltpu.make_async_remote_copy(
            src_ref=y_own.at[col],
            dst_ref=y_part.at[col],
            send_sem=y_sem.at[0, col],
            recv_sem=y_sem.at[1, col],
            device_id=(f, across_y),
            device_id_type=MESH,
        )

    def z_copy(col):
        return pltpu.make_async_remote_copy(
            src_ref=z_own.at[col],
            dst_ref=z_part.at[col],
            send_sem=z_sem.at[0, col],
            recv_sem=z_sem.at[1, col],
            device_id=(partner, t),
            device_id_type=MESH,
        )

    steps = 2 * fs // 2

    def finish(i, carry):
        @pl.when(i == 4)
        def _():
            events(far_out, late, True)

        @pl.when(i < steps)
        def _():
            line, s, far = source_of(i)

            @pl.when(far == 1)
            def _():
                arrived(s, late)

            part[s] = jnp.dot(
                hidden[...], down_all[s], preferred_element_type=jnp.float32
            ).astype(jnp.bfloat16)

            @pl.when(line % 2 != t % 2)
            def _():
                mate_copy(s).start()

        @pl.when((i >= 1) & (i <= steps))
        def _():
            line, s, _ = source_of(i - 1)

            @pl.when(line % 2 == t % 2)
            def _():
                mate_copy(s).wait_recv()

                @pl.when(line != t)
                def _():
                    y_own[s % 2] = (
                        part[s].astype(jnp.float32) + mate_part[s].astype(jnp.float32)
                    ).astype(jnp.bfloat16)
                    y_copy(s % 2).start()

        @pl.when(i >= 2)
        def _():
            line, s, _ = source_of(i - 2)

            @pl.when(line == t)
            def _():
                col = s % 2
                y_copy(col).wait_recv()
                z_own[col] = (
                    part[s, theirs, :].astype(jnp.float32)
                    + mate_part[s, theirs, :].astype(jnp.float32)
                    + y_part[col, theirs, :].astype(jnp.float32)
                ).astype(jnp.bfloat16)
                z_copy(col).start()

        return carry

    lax.fori_loop(0, steps + 2, finish, 0)

    for col in range(2):
        z_copy(col).wait_recv()
        mine = pl.ds(0, tokens)
        s = 2 * t + col
        out_ref[:, col * cols : (col + 1) * cols] = (
            part[s, mine, :].astype(jnp.float32)
            + mate_part[s, mine, :].astype(jnp.float32)
            + y_part[col, mine, :].astype(jnp.float32)
            + z_part[col].astype(jnp.float32)
        ).astype(out_ref.dtype)

    for i in range(2, fs, 2):
        pool_copy(lax.rem(f + i, fs), f).wait_send()
    for i in range(0, fs, 2):
        pool_pass(lax.rem(f + i, fs), pool_ref).wait_send()
    for step in range(4):
        act_finish(step)
    to_partner.wait_send()
    for col in range(2):
        y_copy(col).wait_send()
        z_copy(col).wait_send()

    for k in range(6):
        if k < 3:
            piece(f, k, ACROSS, own(1 - h, k)).wait_send()
        else:

            @pl.when(jnp.logical_not(has_mid))
            def _():
                piece(f, k, ACROSS, own(1 - h, k)).wait_send()

        def rest():
            piece(f, k, MATE).wait_send()
            for line in (a, near, far_in, far_out):
                piece(line * 2 + b, k, MAIN).wait_send()

            @pl.when(inner)
            def _():
                for line in (far_in, far_out):
                    piece(line * 2 + b, k, MATE).wait_send()

        guarded(k, rest)

    def drain(s, carry):
        @pl.when((s // 2) % 2 != t % 2)
        def _():
            mate_copy(s).wait_send()

        return carry

    lax.fori_loop(0, fs, drain, 0)


def body(
    fs,
    tp,
    stream,
    gain_mix,
    pool_weight,
    pool_gain,
    gain_ffn,
    gate_weight,
    up_weight,
    gate_taps,
    up_taps,
    down_weight,
):
    tokens, block = stream.shape
    depth, width = gate_weight.shape
    cols = down_weight.shape[1]
    channels = gain_mix.shape[0]
    t = lax.axis_index("tp")

    def mine(values, size):
        return lax.dynamic_slice_in_dim(values, t * size, size, values.ndim - 1)

    bf16, f32 = jnp.bfloat16, jnp.float32
    dma = pltpu.SemaphoreType.DMA
    split = fs == 8 and tp == 4 and width % 256 == 128 and depth % 16 == 0
    if split:
        held = (width + 128) // 2
        run = split_kernel
        scratch = [
            pltpu.VMEM((fs, depth, held), bf16),
            pltpu.VMEM((fs, depth, held), bf16),
            pltpu.VMEM((fs, held, cols), bf16),
            pltpu.VMEM((fs,) + pool_weight.shape, bf16),
            pltpu.VMEM((tp, 2 * tokens, block), bf16),
            pltpu.VMEM((tp, 2 * tokens, block), bf16),
            pltpu.VMEM((2 * tokens, channels), bf16),
            pltpu.VMEM((channels, block), bf16),
            pltpu.VMEM((2 * tokens, channels), bf16),
            pltpu.VMEM((2 * tokens, held), bf16),
            pltpu.VMEM((2 * tokens, held), bf16),
            pltpu.VMEM((2 * tokens, held), bf16),
            pltpu.VMEM((fs, 2 * tokens, cols), bf16),
            pltpu.VMEM((fs, 2 * tokens, cols), bf16),
            pltpu.VMEM((2, 2 * tokens, cols), bf16),
            pltpu.VMEM((2, 2 * tokens, cols), bf16),
            pltpu.VMEM((2, tokens, cols), bf16),
            pltpu.VMEM((2, tokens, cols), bf16),
            pltpu.VMEM((2 * tokens, block), bf16),
            dma((3, fs, 6)),
            dma((fs, 6)),
            dma((fs,)),
            dma((fs,)),
            dma((4, 3)),
            dma((4, tp)),
            dma((2,)),
            dma((fs,)),
            dma((fs,)),
            dma((2, 2)),
            dma((2, 2)),
            dma((10,)),
        ]
    else:
        run = kernel
        scratch = [
            pltpu.VMEM((fs, depth, width), bf16),
            pltpu.VMEM((fs, depth, width), bf16),
            pltpu.VMEM((fs, width, cols), bf16),
            pltpu.VMEM((fs,) + pool_weight.shape, bf16),
            pltpu.VMEM((tp, tokens, block), bf16),
            pltpu.VMEM((tp, tokens, block), bf16),
            pltpu.VMEM((tokens, channels), bf16),
            pltpu.VMEM((channels, block), bf16),
            pltpu.VMEM((tokens, channels), bf16),
            pltpu.VMEM((tokens, width), f32),
            pltpu.VMEM((tokens, width), f32),
            pltpu.VMEM((tokens, width), bf16),
            pltpu.VMEM((fs, tokens, cols), bf16),
            pltpu.VMEM((tp, 2, tokens, cols), bf16),
            pltpu.VMEM((tokens, block), bf16),
            dma((3, fs, 6)),
            dma((fs, 6)),
            dma((fs,)),
            dma((fs,)),
            dma((2, tp, 2)),
            dma((2, tp)),
            dma((fs,)),
            dma((tp, 2)),
            dma((5,)),
        ]

    def whole(values, size):
        return values if split else mine(values, size)

    return pl.pallas_call(
        functools.partial(run, fs, tp),
        out_shape=jax.ShapeDtypeStruct((tokens, block), bf16),
        in_specs=[pl.BlockSpec(memory_space=pltpu.VMEM)] * 10,
        out_specs=pl.BlockSpec(memory_space=pltpu.VMEM),
        scratch_shapes=scratch,
        compiler_params=pltpu.CompilerParams(
            collective_id=0, has_side_effects=True, vmem_limit_bytes=64 * 1024 * 1024 - 65536
        ),
    )(
        stream,
        gain_mix.reshape(1, channels),
        pool_weight,
        whole(pool_gain, block).reshape(1, -1),
        gain_ffn.reshape(1, channels),
        gate_weight,
        up_weight,
        whole(gate_taps, width),
        whole(up_taps, width),
        down_weight,
    )


def solution(mesh):
    return jax.shard_map(
        functools.partial(body, mesh.shape["fs"], mesh.shape["tp"]),
        mesh=mesh,
        in_specs=(
            P("fs", "tp"),
            P(),
            P(None, "fs", "tp"),
            P(),
            P(),
            P("fs", "tp"),
            P("fs", "tp"),
            P(),
            P(),
            P("tp", "fs"),
        ),
        out_specs=P("fs", "tp"),
        check_vma=False,
    )
```

```python
import functools

import jax
import jax.numpy as jnp
from jax import lax
from jax.experimental import pallas as pl
from jax.experimental.pallas import tpu as pltpu
from jax.sharding import PartitionSpec as P

LEN = 128
GROUPS = 4
MESH = pl.DeviceIdType.MESH
epsilon = 1e-06

EARLY = (0, 1, 2, 3)
LATE = 4
CROSS = 5
FORE, BACK, SIDE = 0, 1, 2


def one_hot(rows, cols, hit):
    r = lax.broadcasted_iota(jnp.int32, (rows, cols), 0)
    c = lax.broadcasted_iota(jnp.int32, (rows, cols), 1)
    return jnp.where(hit(r, c), 1.0, 0.0).astype(jnp.bfloat16)


def delayed(values, amount):
    row = lax.broadcasted_iota(jnp.int32, values.shape, 0)
    return jnp.where(row < amount, 0.0, pltpu.roll(values, amount, 0))


def kernel(
    fs,
    tp,
    stream_ref,
    gain_mix_ref,
    pool_ref,
    pool_gain_ref,
    gain_ffn_ref,
    gate_ref,
    up_ref,
    gate_taps_ref,
    up_taps_ref,
    down_ref,
    out_ref,
    gate_all,
    up_all,
    down_all,
    pool_all,
    stream_all,
    middle_all,
    pooled,
    dense,
    normed_ffn,
    gate_sum,
    value_sum,
    hidden,
    part,
    theirs,
    total,
    w_send,
    w_recv,
    p_send,
    p_recv,
    a_send,
    a_recv,
    r_send,
    r_recv,
    own_sem,
):
    f = lax.axis_index("fs")
    t = lax.axis_index("tp")
    na = fs // 2
    a, b = f // 2, f % 2
    tokens, block = stream_ref.shape
    depth = gate_ref.shape[0]
    seqs = tokens // LEN
    cols = down_ref.shape[1]
    mate = t + 1 - 2 * (t % 2)

    barrier = pltpu.get_barrier_semaphore()
    for i in range(1, fs):
        pl.semaphore_signal(
            barrier, inc=1, device_id=(lax.rem(f + i, fs), t), device_id_type=MESH
        )
    for i in range(1, tp):
        pl.semaphore_signal(
            barrier, inc=1, device_id=(f, lax.rem(t + i, tp)), device_id_type=MESH
        )
    pl.semaphore_wait(barrier, fs + tp - 2)

    def act_copy(step, src, buf, owner, target):
        which = lax.rem(target - t + tp, tp)
        return pltpu.make_async_remote_copy(
            src_ref=src,
            dst_ref=buf.at[owner],
            send_sem=a_send.at[step, which, jnp.where(owner == t, 0, 1)],
            recv_sem=a_recv.at[step, owner],
            device_id=(f, target),
            device_id_type=MESH,
        )

    def act_start(step, src, buf):
        for i in range(2, tp, 2):
            act_copy(step, src, buf, t, lax.rem(t + i, tp)).start()
        act_copy(step, src, buf, t, mate).start()

    def act_relay(step, src, buf):
        for i in range(2, tp, 2):
            owner = lax.rem(t + i, tp)
            act_copy(step, buf.at[owner], buf, owner, mate).wait_recv()
            pltpu.make_async_remote_copy(
                src_ref=buf.at[owner],
                dst_ref=buf.at[owner],
                send_sem=a_send.at[step, i + 1, 1],
                recv_sem=a_recv.at[step, owner],
                device_id=(f, mate),
                device_id_type=MESH,
            ).start()
        for i in range(0, tp, 2):
            owner = lax.rem(mate + i, tp)
            act_copy(step, src, buf, owner, mate).wait_recv()

    def act_finish(step, src, buf):
        for i in range(2, tp, 2):
            act_copy(step, src, buf, t, lax.rem(t + i, tp)).wait_send()
            pltpu.make_async_remote_copy(
                src_ref=src,
                dst_ref=src,
                send_sem=a_send.at[step, i + 1, 1],
                recv_sem=a_recv.at[step, 0],
                device_id=(f, mate),
                device_id_type=MESH,
            ).wait_send()
        act_copy(step, src, buf, t, mate).wait_send()

    def pool_copy(target):
        return pltpu.make_async_remote_copy(
            src_ref=pool_ref,
            dst_ref=pool_all.at[f],
            send_sem=p_send.at[target],
            recv_sem=p_recv.at[f],
            device_id=(target, t),
            device_id_type=MESH,
        )

    act_start(0, stream_ref, stream_all)
    for i in range(1, fs):
        pool_copy(lax.rem(f + i, fs)).start()

    def slot(src, k):
        full = (gate_all, up_all, down_all)[k // 2]
        rows = full.shape[1] // 2
        return full.at[src, pl.ds((k % 2) * rows, rows)]

    def own(k):
        full = (gate_ref, up_ref, down_ref)[k // 2]
        rows = full.shape[0] // 2
        return full.at[pl.ds((k % 2) * rows, rows)]

    def piece(src, k, way, ref=None):
        target = (f + 2, f - 2, f + 1 - 2 * b)[way]
        return pltpu.make_async_remote_copy(
            src_ref=slot(src, k) if ref is None else ref,
            dst_ref=slot(src, k),
            send_sem=w_send.at[way, src, k],
            recv_sem=w_recv.at[src, k],
            device_id=(target, t),
            device_id_type=MESH,
        )

    def along(src, k, ref=None):
        @pl.when(a < na - 1)
        def _():
            piece(src, k, FORE, ref).start()

        @pl.when(a > 0)
        def _():
            piece(src, k, BACK, ref).start()

    pair = f + 1 - 2 * b
    piece(f, CROSS, SIDE, own(CROSS)).start()
    for k in EARLY:
        along(f, k, own(k))
        piece(f, k, SIDE, own(k)).start()
    locals_ = [
        pltpu.make_async_copy(stream_ref, stream_all.at[t], own_sem.at[0]),
        pltpu.make_async_copy(pool_ref, pool_all.at[f], own_sem.at[1]),
        pltpu.make_async_copy(gate_ref, gate_all.at[f], own_sem.at[2]),
        pltpu.make_async_copy(up_ref, up_all.at[f], own_sem.at[3]),
        pltpu.make_async_copy(down_ref, down_all.at[f], own_sem.at[4]),
    ]
    for copy in locals_:
        copy.start()

    def arrive(src, k, way):
        piece(src, k, way).wait_recv()
        if way == FORE:

            @pl.when(a < na - 1)
            def _():
                piece(src, k, FORE).start()

        else:

            @pl.when(a > 0)
            def _():
                piece(src, k, BACK).start()

    def events(d, ks):
        for k in ks:
            for way in (FORE, BACK):
                source = a - d if way == FORE else a + d

                @pl.when((source >= 0) & (source < na))
                def _():
                    src = source * 2 + b
                    arrive(src, k, way)
                    if k == CROSS:
                        arrive(source * 2 + 1 - b, k, way)
                    else:
                        piece(src, k, SIDE).start()

    for i in range(1, fs):
        src = lax.rem(f + i, fs)
        pltpu.make_async_remote_copy(
            src_ref=pool_ref,
            dst_ref=pool_all.at[src],
            send_sem=p_send.at[src],
            recv_sem=p_recv.at[src],
            device_id=(src, t),
            device_id_type=MESH,
        ).wait_recv()
    for copy in locals_:
        copy.wait()
    _, chans, outs = pool_ref.shape
    spread_rows = one_hot(
        GROUPS * chans,
        GROUPS * chans,
        lambda r, c: c == (r % GROUPS) * chans + r // GROUPS,
    )
    spread_cols = [
        one_hot(outs, GROUPS * outs, lambda r, c, g=g: c == r * GROUPS + g)
        for g in range(GROUPS)
    ]

    def densify(s, carry):
        wide = jnp.concatenate(
            [
                jnp.dot(
                    pool_all[s, g], spread_cols[g], preferred_element_type=jnp.float32
                )
                for g in range(GROUPS)
            ],
            axis=0,
        ).astype(jnp.bfloat16)
        rows = pl.ds(pl.multiple_of(s * GROUPS * chans, GROUPS * chans), GROUPS * chans)
        dense[rows, :] = jnp.dot(
            spread_rows, wide, preferred_element_type=jnp.float32
        ).astype(jnp.bfloat16)
        return carry

    lax.fori_loop(0, fs, densify, 0)

    act_relay(0, stream_ref, stream_all)

    def factor(buf, rows):
        square = jnp.zeros((LEN, 1), jnp.float32)
        for i in range(tp):
            v = buf[i, rows, :].astype(jnp.float32)
            square = square + jnp.sum(v * v, axis=-1, keepdims=True)
        return lax.rsqrt(square / (tp * block) + epsilon)

    def pool_seq(q, carry):
        rows = pl.ds(pl.multiple_of(q * LEN, LEN), LEN)
        scale = factor(stream_all, rows)
        lane = lax.broadcasted_iota(jnp.int32, (LEN, block), 1) % GROUPS
        row = lax.broadcasted_iota(jnp.int32, (LEN, block), 0)
        extent = jnp.where(lane == 0, 2, jnp.where(lane == 1, 4, jnp.where(lane == 2, 8, 16)))
        divisor = jnp.minimum(row + 1, extent).astype(jnp.float32)
        for i in range(tp):
            v = stream_all[i, rows, :].astype(jnp.float32)
            v = v * scale * gain_mix_ref[:, i * block : (i + 1) * block]
            v = v.astype(jnp.bfloat16).astype(jnp.float32)
            running = v + delayed(v, 1)
            picked = running
            for g, amount in ((1, 2), (2, 4), (3, 8)):
                running = running + delayed(running, amount)
                picked = jnp.where(lane >= g, running, picked)
            pooled[rows, i * block : (i + 1) * block] = (picked / divisor - v).astype(
                jnp.bfloat16
            )
        return carry

    lax.fori_loop(0, seqs, pool_seq, 0)

    def mix_seq(q, carry):
        rows = pl.ds(pl.multiple_of(q * LEN, LEN), LEN)
        mixed = jnp.dot(pooled[rows, :], dense[...], preferred_element_type=jnp.float32)
        total[rows, :] = (
            stream_ref[rows, :].astype(jnp.float32) + mixed * pool_gain_ref[...]
        ).astype(jnp.bfloat16)
        return carry

    lax.fori_loop(0, seqs, mix_seq, 0)

    act_start(1, total, middle_all)
    keep = pltpu.make_async_copy(total, middle_all.at[t], own_sem.at[0])
    keep.start()
    events(1, EARLY)
    gate_sum[...] = jnp.zeros_like(gate_sum)
    value_sum[...] = jnp.zeros_like(value_sum)
    keep.wait()
    act_relay(1, total, middle_all)

    def norm_seq(q, carry):
        rows = pl.ds(pl.multiple_of(q * LEN, LEN), LEN)
        scale = factor(middle_all, rows)
        for i in range(tp):
            span = slice(i * block, (i + 1) * block)
            v = middle_all[i, rows, :].astype(jnp.float32)
            normed_ffn[rows, span] = (v * scale * gain_ffn_ref[:, span]).astype(jnp.bfloat16)
        return carry

    lax.fori_loop(0, seqs, norm_seq, 0)

    def sources(d, take):
        def one(i, carry):
            far, up = i // 2, i % 2
            dist = d - far
            source = a + (2 * up - 1) * dist
            src = source * 2 + b + far - 2 * b * far
            exists = (source >= 0) & (source < na) & (dist >= 0) & (dist < na)

            @pl.when(exists & ((dist > 0) | (up == 0)))
            def _():
                take(src, source, far)

            return carry

        lax.fori_loop(0, 4, one, 0)

    half = tokens // 2

    def project(src, source, far):
        @pl.when(far == 1)
        def _():
            for k in EARLY:
                piece(src, k, SIDE).wait_recv()

        span = pl.ds(pl.multiple_of(src * depth, depth), depth)

        def chunk(m, carry):
            rows = pl.ds(pl.multiple_of(m * half, half), half)
            left = normed_ffn[rows, span]
            gate_sum[rows, :] += jnp.dot(
                left, gate_all[src], preferred_element_type=jnp.float32
            )
            value_sum[rows, :] += jnp.dot(
                left, up_all[src], preferred_element_type=jnp.float32
            )
            return carry

        lax.fori_loop(0, 2, chunk, 0)

    def late_start():
        along(f, LATE, own(LATE))
        piece(f, LATE, SIDE, own(LATE)).start()
        along(f, CROSS, own(CROSS))
        piece(pair, CROSS, SIDE).wait_recv()
        along(pair, CROSS)

    def early_round(d, carry):
        @pl.when((d >= 1) & (d <= na - 2))
        def _():
            events(d + 1, EARLY)

        @pl.when(d == na - 2)
        def _():
            late_start()

        @pl.when(d >= na - 1)
        def _():
            events(d - na + 2, (LATE, CROSS))

        sources(d, project)
        return carry

    lax.fori_loop(0, na + 1, early_round, 0)

    def gate_seq(q, carry):
        rows = pl.ds(pl.multiple_of(q * LEN, LEN), LEN)

        def conv(sums, taps):
            v = sums[rows, :].astype(jnp.bfloat16).astype(jnp.float32)
            reach = taps.shape[0]
            running = v * taps[reach - 1 : reach, :]
            for i in range(1, reach):
                running = running + delayed(v, i) * taps[reach - 1 - i : reach - i, :]
            return running

        gate = conv(gate_sum, gate_taps_ref)
        value = conv(value_sum, up_taps_ref)
        hidden[rows, :] = (gate / (1.0 + jnp.exp(-gate)) * value).astype(jnp.bfloat16)
        return carry

    lax.fori_loop(0, seqs, gate_seq, 0)

    def part_copy(src, source, col):
        return pltpu.make_async_remote_copy(
            src_ref=part.at[src],
            dst_ref=theirs.at[t, col],
            send_sem=r_send.at[src],
            recv_sem=r_recv.at[t, col],
            device_id=(f, source),
            device_id_type=MESH,
        )

    def finish(src, source, far):
        @pl.when(far == 1)
        def _():
            piece(src, LATE, SIDE).wait_recv()

        part[src] = jnp.dot(
            hidden[...], down_all[src], preferred_element_type=jnp.float32
        ).astype(jnp.bfloat16)

        @pl.when(source != t)
        def _():
            part_copy(src, source, src % 2).start()

    def late_round(d, carry):
        @pl.when((d >= 2) & (d + 1 < na))
        def _():
            events(d + 1, (LATE,))

        @pl.when((d >= 3) & (d < na))
        def _():
            events(d, (CROSS,))

        sources(d, finish)
        return carry

    lax.fori_loop(0, na + 1, late_round, 0)

    for col in range(2):
        for i in range(1, tp):
            peer = lax.rem(t + i, tp)
            pltpu.make_async_remote_copy(
                src_ref=part.at[0],
                dst_ref=theirs.at[peer, col],
                send_sem=r_send.at[0],
                recv_sem=r_recv.at[peer, col],
                device_id=(f, peer),
                device_id_type=MESH,
            ).wait_recv()
        summed = part[2 * t + col].astype(jnp.float32)
        for i in range(1, tp):
            summed = summed + theirs[lax.rem(t + i, tp), col].astype(jnp.float32)
        out_ref[:, col * cols : (col + 1) * cols] = summed.astype(out_ref.dtype)

    for i in range(1, fs):
        pool_copy(lax.rem(f + i, fs)).wait_send()
    act_finish(0, stream_ref, stream_all)
    act_finish(1, total, middle_all)

    def drain(s, carry):
        for k in range(6):
            line, col = s // 2, s % 2
            mine = (col == b) | (k == CROSS)

            @pl.when(mine & (a < na - 1) & (line <= a))
            def _():
                piece(s, k, FORE).wait_send()

            @pl.when(mine & (a > 0) & (line >= a))
            def _():
                piece(s, k, BACK).wait_send()

            @pl.when((s == f) if k == CROSS else (col == b))
            def _():
                piece(s, k, SIDE).wait_send()

        @pl.when(s // 2 != t)
        def _():
            part_copy(s, s // 2, s % 2).wait_send()

        return carry

    lax.fori_loop(0, fs, drain, 0)


MAIN, MATE, ACROSS = 0, 1, 2


def split_kernel(
    fs,
    tp,
    stream_ref,
    gain_mix_ref,
    pool_ref,
    pool_gain_ref,
    gain_ffn_ref,
    gate_ref,
    up_ref,
    gate_taps_ref,
    up_taps_ref,
    down_ref,
    out_ref,
    gate_all,
    up_all,
    down_all,
    pool_all,
    stream_all,
    middle_all,
    pooled,
    dense,
    normed_ffn,
    gate_sum,
    value_sum,
    hidden,
    part,
    mate_part,
    y_own,
    y_part,
    z_own,
    z_part,
    total,
    w_send,
    w_recv,
    p_send,
    p_recv,
    a_send,
    a_recv,
    b_sem,
    m_send,
    m_recv,
    y_sem,
    z_sem,
    own_sem,
):
    f = lax.axis_index("fs")
    t = lax.axis_index("tp")
    a, b = f // 2, f % 2
    tokens, block = stream_ref.shape
    depth, width = gate_ref.shape
    held = gate_all.shape[2]
    other = width - held
    seqs = tokens // LEN
    cols = down_ref.shape[1]
    mate = t + 1 - 2 * (t % 2)
    across_y = lax.rem(t + 2, tp)
    h = a // 2
    has_mid = t % 2 == h
    near = a + 1 - 2 * (a % 2)
    far_in, far_out = 2 - h, 3 * (1 - h)
    inner = (a == 1) | (a == 2)
    first = jnp.where(inner, far_in, near)
    second = jnp.where(inner, far_out, far_in)
    third = jnp.where(inner, near, far_out)
    partner = lax.rem(f + fs // 2, fs)
    pair = f + 1 - 2 * b

    barrier = pltpu.get_barrier_semaphore()
    for i in range(1, fs):
        pl.semaphore_signal(
            barrier, inc=1, device_id=(lax.rem(f + i, fs), t), device_id_type=MESH
        )
    for i in range(1, tp):
        pl.semaphore_signal(
            barrier, inc=1, device_id=(f, lax.rem(t + i, tp)), device_id_type=MESH
        )
    pl.semaphore_wait(barrier, fs + tp - 2)

    def act_view(step):
        buf = stream_all if step < 2 else middle_all
        return lambda owner: buf.at[owner, pl.ds((step % 2) * tokens, tokens)]

    def act_copy(step, src, owner, target, role):
        return pltpu.make_async_remote_copy(
            src_ref=src,
            dst_ref=act_view(step)(owner),
            send_sem=a_send.at[step, role],
            recv_sem=a_recv.at[step, owner],
            device_id=(f, target),
            device_id_type=MESH,
        )

    def act_start(step, src):
        act_copy(step, src, t, across_y, 0).start()
        act_copy(step, src, t, mate, 1).start()

    def act_relay(step):
        view = act_view(step)
        act_copy(step, view(across_y), across_y, mate, 2).wait_recv()
        act_copy(step, view(across_y), across_y, mate, 2).start()
        act_copy(step, view(mate), mate, mate, 2).wait_recv()
        diagonal = lax.rem(mate + 2, tp)
        act_copy(step, view(diagonal), diagonal, mate, 2).wait_recv()

    def act_finish(step):
        view = act_view(step)
        for role in range(3):
            act_copy(step, view(t), t, mate, role).wait_send()

    def pool_copy(target, owner):
        return pltpu.make_async_remote_copy(
            src_ref=pool_ref,
            dst_ref=pool_all.at[owner],
            send_sem=p_send.at[target],
            recv_sem=p_recv.at[owner],
            device_id=(target, t),
            device_id_type=MESH,
        )

    to_partner = pltpu.make_async_remote_copy(
        src_ref=stream_ref,
        dst_ref=stream_all.at[t, pl.ds(tokens, tokens)],
        send_sem=b_sem.at[0],
        recv_sem=b_sem.at[1],
        device_id=(partner, t),
        device_id_type=MESH,
    )

    def pool_pass(owner, ref):
        return pltpu.make_async_remote_copy(
            src_ref=ref,
            dst_ref=pool_all.at[owner],
            send_sem=p_send.at[owner // 2 * 2 + 1 - b],
            recv_sem=p_recv.at[owner],
            device_id=(pair, t),
            device_id_type=MESH,
        )

    act_start(0, stream_ref)
    for i in range(2, fs, 2):
        pool_copy(lax.rem(f + i, fs), f).start()
    pool_pass(f, pool_ref).start()

    def slot(src, k):
        full = (gate_all, up_all, down_all)[k % 3]
        span = pl.ds(0, other) if k < 3 else pl.ds(other, held - other)
        if k % 3 == 2:
            return full.at[src, span]
        return full.at[src, :, span]

    def own(q, k):
        full = (gate_ref, up_ref, down_ref)[k % 3]
        if k < 3:
            span = pl.ds(pl.multiple_of(q * held, 128), other)
        else:
            span = pl.ds(other, held - other)
        if k % 3 == 2:
            return full.at[span]
        return full.at[:, span]

    def piece(src, k, way, ref=None):
        target = (pair, near * 2 + b, far_in * 2 + b)[way]
        return pltpu.make_async_remote_copy(
            src_ref=slot(src, k) if ref is None else ref,
            dst_ref=slot(src, k),
            send_sem=w_send.at[way, src, k],
            recv_sem=w_recv.at[src, k],
            device_id=(target, t),
            device_id_type=MESH,
        )

    def guarded(k, do):
        if k < 3:
            do()
        else:
            pl.when(has_mid)(do)

    def own_across(k):
        if k < 3:
            piece(f, k, ACROSS, own(1 - h, k)).start()
        else:

            @pl.when(jnp.logical_not(has_mid))
            def _():
                piece(f, k, ACROSS, own(1 - h, k)).start()

    def own_near(k):
        guarded(k, lambda: piece(f, k, MATE, own(h, k)).start())

    def own_pair(k):
        guarded(k, lambda: piece(f, k, MAIN, own(h, k)).start())

    def events(source, ks):
        src = source * 2 + b
        for k in ks:

            def one():
                piece(src, k, MAIN).wait_recv()

                @pl.when(inner & (source // 2 != h))
                def _():
                    piece(src, k, MATE).start()

                piece(src, k, MAIN).start()

            guarded(k, one)

    def arrived(src, ks):
        for k in ks:
            guarded(k, lambda: piece(src, k, MAIN).wait_recv())

    early, late = (0, 3, 1, 4), (2, 5)
    own_pair(early[0])

    def local(k):
        return pltpu.make_async_copy(own(h, k), slot(f, k), own_sem.at[k])

    for k in range(6):
        guarded(k, lambda: local(k).start())
    keep_stream = pltpu.make_async_copy(
        stream_ref, stream_all.at[t, pl.ds(0, tokens)], own_sem.at[6]
    )
    keep_pool = pltpu.make_async_copy(pool_ref, pool_all.at[f], own_sem.at[7])
    keep_stream.start()
    keep_pool.start()

    @pl.when(jnp.logical_not(has_mid))
    def _():
        gate_all[:, :, other:] = jnp.zeros((fs, depth, held - other), jnp.bfloat16)
        up_all[:, :, other:] = jnp.zeros((fs, depth, held - other), jnp.bfloat16)
        down_all[:, other:, :] = jnp.zeros((fs, held - other, cols), jnp.bfloat16)

    for i in range(2, fs, 2):
        src = lax.rem(f + i, fs)
        pool_copy(src, src).wait_recv()
        pool_pass(src, pool_all.at[src]).start()
    to_partner.start()
    for k in early:
        own_across(k)

    @pl.when(inner)
    def _():
        for k in early:
            own_near(k)

    for k in early[1:]:
        own_pair(k)
    for i in range(0, fs, 2):
        src = lax.rem(pair + i, fs)
        pool_copy(src, src).wait_recv()
    keep_pool.wait()
    _, chans, outs = pool_ref.shape
    spread_rows = one_hot(
        GROUPS * chans,
        GROUPS * chans,
        lambda r, c: c == (r % GROUPS) * chans + r // GROUPS,
    )
    spread_cols = [
        one_hot(outs, GROUPS * outs, lambda r, c, g=g: c == r * GROUPS + g)
        for g in range(GROUPS)
    ]

    def densify(s, carry):
        wide = jnp.concatenate(
            [
                jnp.dot(
                    pool_all[s, g], spread_cols[g], preferred_element_type=jnp.float32
                )
                for g in range(GROUPS)
            ],
            axis=0,
        ).astype(jnp.bfloat16)
        rows = pl.ds(pl.multiple_of(s * GROUPS * chans, GROUPS * chans), GROUPS * chans)
        dense[rows, :] = jnp.dot(
            spread_rows, wide, preferred_element_type=jnp.float32
        ).astype(jnp.bfloat16)
        return carry

    lax.fori_loop(0, fs, densify, 0)
    keep_stream.wait()
    act_relay(0)

    def factor(buf, rows):
        square = jnp.zeros((LEN, 1), jnp.float32)
        for i in range(tp):
            v = buf[i, rows, :].astype(jnp.float32)
            square = square + jnp.sum(v * v, axis=-1, keepdims=True)
        return lax.rsqrt(square / (tp * block) + epsilon)

    def pool_seq(q, carry):
        rows = pl.ds(pl.multiple_of(q * LEN, LEN), LEN)
        scale = factor(stream_all, rows)
        lane = lax.broadcasted_iota(jnp.int32, (LEN, block), 1) % GROUPS
        row = lax.broadcasted_iota(jnp.int32, (LEN, block), 0)
        extent = jnp.where(lane == 0, 2, jnp.where(lane == 1, 4, jnp.where(lane == 2, 8, 16)))
        divisor = jnp.minimum(row + 1, extent).astype(jnp.float32)
        for i in range(tp):
            v = stream_all[i, rows, :].astype(jnp.float32)
            v = v * scale * gain_mix_ref[:, i * block : (i + 1) * block]
            v = v.astype(jnp.bfloat16).astype(jnp.float32)
            running = v + delayed(v, 1)
            picked = running
            for g, amount in ((1, 2), (2, 4), (3, 8)):
                running = running + delayed(running, amount)
                picked = jnp.where(lane >= g, running, picked)
            pooled[rows, i * block : (i + 1) * block] = (picked / divisor - v).astype(
                jnp.bfloat16
            )
        mixed = jnp.dot(pooled[rows, :], dense[...], preferred_element_type=jnp.float32)
        total[rows, :] = (
            stream_all[t, rows, :].astype(jnp.float32)
            + mixed * pool_gain_ref[:, pl.ds(pl.multiple_of(t * block, 128), block)]
        ).astype(jnp.bfloat16)
        return carry

    lax.fori_loop(0, seqs, pool_seq, 0)
    ours, theirs = pl.ds(0, tokens), pl.ds(tokens, tokens)
    act_start(2, total.at[ours])
    keep = [
        pltpu.make_async_copy(total.at[span], middle_all.at[t, span], own_sem.at[8 + i])
        for i, span in enumerate((ours, theirs))
    ]
    keep[0].start()

    @pl.when(jnp.logical_not(inner))
    def _():
        for k in early:
            own_near(k)

    to_partner.wait_recv()
    act_start(1, stream_all.at[t, theirs])
    events(first, early)

    @pl.when(inner)
    def _():
        events(second, early)

    for k in late:
        own_across(k)

    act_relay(1)
    lax.fori_loop(seqs, 2 * seqs, pool_seq, 0)
    act_start(3, total.at[theirs])
    keep[1].start()
    keep[0].wait()
    act_relay(2)

    def norm(first):
        def norm_seq(q, carry):
            rows = pl.ds(pl.multiple_of(first + q * LEN, LEN), LEN)
            scale = factor(middle_all, rows)
            for i in range(tp):
                span = slice(i * block, (i + 1) * block)
                v = middle_all[i, rows, :].astype(jnp.float32)
                normed_ffn[rows, span] = (v * scale * gain_ffn_ref[:, span]).astype(
                    jnp.bfloat16
                )
            return carry

        lax.fori_loop(0, seqs, norm_seq, 0)


    @pl.when(jnp.logical_not(inner))
    def _():
        events(second, early)

    for k in late:
        own_near(k)
        own_pair(k)
    norm(0)
    keep[1].wait()
    act_relay(3)
    norm(tokens)
    events(third, early)
    for k in range(6):
        guarded(k, lambda: local(k).wait())
    arrived(pair, early)
    for source in (near, far_in, far_out):
        arrived(source * 2 + 1 - b, early)

    chunk = 2 * LEN

    def project(m, carry):
        rows = pl.ds(pl.multiple_of(m * chunk, chunk), chunk)
        left = normed_ffn[rows, :]
        for full, sums in ((gate_all, gate_sum), (up_all, value_sum)):
            sums[rows, :] = jnp.dot(
                left,
                full[...].reshape(fs * depth, held),
                preferred_element_type=jnp.float32,
            ).astype(jnp.bfloat16)
        return carry

    def gate_seq(q, carry):
        rows = pl.ds(pl.multiple_of(q * LEN, LEN), LEN)

        def conv(sums, taps_ref):
            taps = jnp.concatenate(
                [
                    taps_ref[:, pl.ds(pl.multiple_of(t * width + h * held, 128), other)],
                    taps_ref[:, pl.ds(pl.multiple_of(t * width + other, 128), held - other)],
                ],
                axis=1,
            )
            v = sums[rows, :].astype(jnp.float32)
            reach = taps.shape[0]
            running = v * taps[reach - 1 : reach, :]
            for i in range(1, reach):
                running = running + delayed(v, i) * taps[reach - 1 - i : reach - i, :]
            return running

        gate = conv(gate_sum, gate_taps_ref)
        value = conv(value_sum, up_taps_ref)
        hidden[rows, :] = (gate / (1.0 + jnp.exp(-gate)) * value).astype(jnp.bfloat16)
        return carry

    chunks = tokens // chunk
    lax.fori_loop(0, chunks, project, 0)
    events(first, late)
    lax.fori_loop(chunks, 2 * chunks, project, 0)
    events(second, late)
    lax.fori_loop(0, 2 * seqs, gate_seq, 0)

    def source_of(i):
        far = jnp.where((i == 2) | (i == 4) | (i == 5) | (i == 7), 1, 0)
        line = jnp.where(
            (i == 0) | (i == 2),
            a,
            jnp.where((i == 3) | (i == 4), first, jnp.where(i >= 6, third, second)),
        )
        return line, line * 2 + b + far - 2 * b * far, far

    def mate_copy(s):
        return pltpu.make_async_remote_copy(
            src_ref=part.at[s],
            dst_ref=mate_part.at[s],
            send_sem=m_send.at[s],
            recv_sem=m_recv.at[s],
            device_id=(f, mate),
            device_id_type=MESH,
        )

    def y_copy(col):
        return pltpu.make_async_remote_copy(
            src_ref=y_own.at[col],
            dst_ref=y_part.at[col],
            send_sem=y_sem.at[0, col],
            recv_sem=y_sem.at[1, col],
            device_id=(f, across_y),
            device_id_type=MESH,
        )

    def z_copy(col):
        return pltpu.make_async_remote_copy(
            src_ref=z_own.at[col],
            dst_ref=z_part.at[col],
            send_sem=z_sem.at[0, col],
            recv_sem=z_sem.at[1, col],
            device_id=(partner, t),
            device_id_type=MESH,
        )

    steps = 2 * fs // 2

    def finish(i, carry):
        @pl.when(i == 4)
        def _():
            events(third, late)

        @pl.when(i < steps)
        def _():
            line, s, far = source_of(i)

            @pl.when(far == 1)
            def _():
                arrived(s, late)

            part[s] = jnp.dot(
                hidden[...], down_all[s], preferred_element_type=jnp.float32
            ).astype(jnp.bfloat16)

            @pl.when(line % 2 != t % 2)
            def _():
                mate_copy(s).start()

        @pl.when((i >= 1) & (i <= steps))
        def _():
            line, s, _ = source_of(i - 1)

            @pl.when(line % 2 == t % 2)
            def _():
                mate_copy(s).wait_recv()

                @pl.when(line != t)
                def _():
                    y_own[s % 2] = (
                        part[s].astype(jnp.float32) + mate_part[s].astype(jnp.float32)
                    ).astype(jnp.bfloat16)
                    y_copy(s % 2).start()

        @pl.when(i >= 2)
        def _():
            line, s, _ = source_of(i - 2)

            @pl.when(line == t)
            def _():
                col = s % 2
                y_copy(col).wait_recv()
                z_own[col] = (
                    part[s, theirs, :].astype(jnp.float32)
                    + mate_part[s, theirs, :].astype(jnp.float32)
                    + y_part[col, theirs, :].astype(jnp.float32)
                ).astype(jnp.bfloat16)
                z_copy(col).start()

        return carry

    lax.fori_loop(0, steps + 2, finish, 0)

    for col in range(2):
        z_copy(col).wait_recv()
        mine = pl.ds(0, tokens)
        s = 2 * t + col
        out_ref[:, col * cols : (col + 1) * cols] = (
            part[s, mine, :].astype(jnp.float32)
            + mate_part[s, mine, :].astype(jnp.float32)
            + y_part[col, mine, :].astype(jnp.float32)
            + z_part[col].astype(jnp.float32)
        ).astype(out_ref.dtype)

    for i in range(2, fs, 2):
        pool_copy(lax.rem(f + i, fs), f).wait_send()
    for i in range(0, fs, 2):
        pool_pass(lax.rem(f + i, fs), pool_ref).wait_send()
    for step in range(4):
        act_finish(step)
    to_partner.wait_send()
    for col in range(2):
        y_copy(col).wait_send()
        z_copy(col).wait_send()

    for k in range(6):
        if k < 3:
            piece(f, k, ACROSS, own(1 - h, k)).wait_send()
        else:

            @pl.when(jnp.logical_not(has_mid))
            def _():
                piece(f, k, ACROSS, own(1 - h, k)).wait_send()

        def rest():
            piece(f, k, MATE).wait_send()
            for line in (a, near, far_in, far_out):
                piece(line * 2 + b, k, MAIN).wait_send()

            @pl.when(inner)
            def _():
                for line in (far_in, far_out):
                    piece(line * 2 + b, k, MATE).wait_send()

        guarded(k, rest)

    def drain(s, carry):
        @pl.when((s // 2) % 2 != t % 2)
        def _():
            mate_copy(s).wait_send()

        return carry

    lax.fori_loop(0, fs, drain, 0)


def body(
    fs,
    tp,
    stream,
    gain_mix,
    pool_weight,
    pool_gain,
    gain_ffn,
    gate_weight,
    up_weight,
    gate_taps,
    up_taps,
    down_weight,
):
    tokens, block = stream.shape
    depth, width = gate_weight.shape
    cols = down_weight.shape[1]
    channels = gain_mix.shape[0]
    t = lax.axis_index("tp")

    def mine(values, size):
        return lax.dynamic_slice_in_dim(values, t * size, size, values.ndim - 1)

    bf16, f32 = jnp.bfloat16, jnp.float32
    dma = pltpu.SemaphoreType.DMA
    split = fs == 8 and tp == 4 and width % 256 == 128 and depth % 16 == 0
    if split:
        held = (width + 128) // 2
        run = split_kernel
        scratch = [
            pltpu.VMEM((fs, depth, held), bf16),
            pltpu.VMEM((fs, depth, held), bf16),
            pltpu.VMEM((fs, held, cols), bf16),
            pltpu.VMEM((fs,) + pool_weight.shape, bf16),
            pltpu.VMEM((tp, 2 * tokens, block), bf16),
            pltpu.VMEM((tp, 2 * tokens, block), bf16),
            pltpu.VMEM((2 * tokens, channels), bf16),
            pltpu.VMEM((channels, block), bf16),
            pltpu.VMEM((2 * tokens, channels), bf16),
            pltpu.VMEM((2 * tokens, held), bf16),
            pltpu.VMEM((2 * tokens, held), bf16),
            pltpu.VMEM((2 * tokens, held), bf16),
            pltpu.VMEM((fs, 2 * tokens, cols), bf16),
            pltpu.VMEM((fs, 2 * tokens, cols), bf16),
            pltpu.VMEM((2, 2 * tokens, cols), bf16),
            pltpu.VMEM((2, 2 * tokens, cols), bf16),
            pltpu.VMEM((2, tokens, cols), bf16),
            pltpu.VMEM((2, tokens, cols), bf16),
            pltpu.VMEM((2 * tokens, block), bf16),
            dma((3, fs, 6)),
            dma((fs, 6)),
            dma((fs,)),
            dma((fs,)),
            dma((4, 3)),
            dma((4, tp)),
            dma((2,)),
            dma((fs,)),
            dma((fs,)),
            dma((2, 2)),
            dma((2, 2)),
            dma((10,)),
        ]
    else:
        run = kernel
        scratch = [
            pltpu.VMEM((fs, depth, width), bf16),
            pltpu.VMEM((fs, depth, width), bf16),
            pltpu.VMEM((fs, width, cols), bf16),
            pltpu.VMEM((fs,) + pool_weight.shape, bf16),
            pltpu.VMEM((tp, tokens, block), bf16),
            pltpu.VMEM((tp, tokens, block), bf16),
            pltpu.VMEM((tokens, channels), bf16),
            pltpu.VMEM((channels, block), bf16),
            pltpu.VMEM((tokens, channels), bf16),
            pltpu.VMEM((tokens, width), f32),
            pltpu.VMEM((tokens, width), f32),
            pltpu.VMEM((tokens, width), bf16),
            pltpu.VMEM((fs, tokens, cols), bf16),
            pltpu.VMEM((tp, 2, tokens, cols), bf16),
            pltpu.VMEM((tokens, block), bf16),
            dma((3, fs, 6)),
            dma((fs, 6)),
            dma((fs,)),
            dma((fs,)),
            dma((2, tp, 2)),
            dma((2, tp)),
            dma((fs,)),
            dma((tp, 2)),
            dma((5,)),
        ]

    def whole(values, size):
        return values if split else mine(values, size)

    return pl.pallas_call(
        functools.partial(run, fs, tp),
        out_shape=jax.ShapeDtypeStruct((tokens, block), bf16),
        in_specs=[pl.BlockSpec(memory_space=pltpu.VMEM)] * 10,
        out_specs=pl.BlockSpec(memory_space=pltpu.VMEM),
        scratch_shapes=scratch,
        compiler_params=pltpu.CompilerParams(
            collective_id=0, has_side_effects=True, vmem_limit_bytes=64 * 1024 * 1024 - 65536
        ),
    )(
        stream,
        gain_mix.reshape(1, channels),
        pool_weight,
        whole(pool_gain, block).reshape(1, -1),
        gain_ffn.reshape(1, channels),
        gate_weight,
        up_weight,
        whole(gate_taps, width),
        whole(up_taps, width),
        down_weight,
    )


def solution(mesh):
    return jax.shard_map(
        functools.partial(body, mesh.shape["fs"], mesh.shape["tp"]),
        mesh=mesh,
        in_specs=(
            P("fs", "tp"),
            P(),
            P(None, "fs", "tp"),
            P(),
            P(),
            P("fs", "tp"),
            P("fs", "tp"),
            P(),
            P(),
            P("tp", "fs"),
        ),
        out_specs=P("fs", "tp"),
        check_vma=False,
    )
```

```python
import functools

import jax
import jax.numpy as jnp
from jax import lax
from jax.experimental import pallas as pl
from jax.experimental.pallas import tpu as pltpu
from jax.sharding import PartitionSpec as P

LEN = 128
GROUPS = 4
MESH = pl.DeviceIdType.MESH
epsilon = 1e-06

EARLY = (0, 1, 2, 3)
LATE = 4
CROSS = 5
FORE, BACK, SIDE = 0, 1, 2


def one_hot(rows, cols, hit):
    r = lax.broadcasted_iota(jnp.int32, (rows, cols), 0)
    c = lax.broadcasted_iota(jnp.int32, (rows, cols), 1)
    return jnp.where(hit(r, c), 1.0, 0.0).astype(jnp.bfloat16)


def delayed(values, amount):
    row = lax.broadcasted_iota(jnp.int32, values.shape, 0)
    return jnp.where(row < amount, 0.0, pltpu.roll(values, amount, 0))


def kernel(
    fs,
    tp,
    stream_ref,
    gain_mix_ref,
    pool_ref,
    pool_gain_ref,
    gain_ffn_ref,
    gate_ref,
    up_ref,
    gate_taps_ref,
    up_taps_ref,
    down_ref,
    out_ref,
    gate_all,
    up_all,
    down_all,
    pool_all,
    stream_all,
    middle_all,
    pooled,
    dense,
    normed_ffn,
    gate_sum,
    value_sum,
    hidden,
    part,
    theirs,
    total,
    w_send,
    w_recv,
    p_send,
    p_recv,
    a_send,
    a_recv,
    r_send,
    r_recv,
    own_sem,
):
    f = lax.axis_index("fs")
    t = lax.axis_index("tp")
    na = fs // 2
    a, b = f // 2, f % 2
    tokens, block = stream_ref.shape
    depth = gate_ref.shape[0]
    seqs = tokens // LEN
    cols = down_ref.shape[1]
    mate = t + 1 - 2 * (t % 2)

    barrier = pltpu.get_barrier_semaphore()
    for i in range(1, fs):
        pl.semaphore_signal(
            barrier, inc=1, device_id=(lax.rem(f + i, fs), t), device_id_type=MESH
        )
    for i in range(1, tp):
        pl.semaphore_signal(
            barrier, inc=1, device_id=(f, lax.rem(t + i, tp)), device_id_type=MESH
        )
    pl.semaphore_wait(barrier, fs + tp - 2)

    def act_copy(step, src, buf, owner, target):
        which = lax.rem(target - t + tp, tp)
        return pltpu.make_async_remote_copy(
            src_ref=src,
            dst_ref=buf.at[owner],
            send_sem=a_send.at[step, which, jnp.where(owner == t, 0, 1)],
            recv_sem=a_recv.at[step, owner],
            device_id=(f, target),
            device_id_type=MESH,
        )

    def act_start(step, src, buf):
        for i in range(2, tp, 2):
            act_copy(step, src, buf, t, lax.rem(t + i, tp)).start()
        act_copy(step, src, buf, t, mate).start()

    def act_relay(step, src, buf):
        for i in range(2, tp, 2):
            owner = lax.rem(t + i, tp)
            act_copy(step, buf.at[owner], buf, owner, mate).wait_recv()
            pltpu.make_async_remote_copy(
                src_ref=buf.at[owner],
                dst_ref=buf.at[owner],
                send_sem=a_send.at[step, i + 1, 1],
                recv_sem=a_recv.at[step, owner],
                device_id=(f, mate),
                device_id_type=MESH,
            ).start()
        for i in range(0, tp, 2):
            owner = lax.rem(mate + i, tp)
            act_copy(step, src, buf, owner, mate).wait_recv()

    def act_finish(step, src, buf):
        for i in range(2, tp, 2):
            act_copy(step, src, buf, t, lax.rem(t + i, tp)).wait_send()
            pltpu.make_async_remote_copy(
                src_ref=src,
                dst_ref=src,
                send_sem=a_send.at[step, i + 1, 1],
                recv_sem=a_recv.at[step, 0],
                device_id=(f, mate),
                device_id_type=MESH,
            ).wait_send()
        act_copy(step, src, buf, t, mate).wait_send()

    def pool_copy(target):
        return pltpu.make_async_remote_copy(
            src_ref=pool_ref,
            dst_ref=pool_all.at[f],
            send_sem=p_send.at[target],
            recv_sem=p_recv.at[f],
            device_id=(target, t),
            device_id_type=MESH,
        )

    act_start(0, stream_ref, stream_all)
    for i in range(1, fs):
        pool_copy(lax.rem(f + i, fs)).start()

    def slot(src, k):
        full = (gate_all, up_all, down_all)[k // 2]
        rows = full.shape[1] // 2
        return full.at[src, pl.ds((k % 2) * rows, rows)]

    def own(k):
        full = (gate_ref, up_ref, down_ref)[k // 2]
        rows = full.shape[0] // 2
        return full.at[pl.ds((k % 2) * rows, rows)]

    def piece(src, k, way, ref=None):
        target = (f + 2, f - 2, f + 1 - 2 * b)[way]
        return pltpu.make_async_remote_copy(
            src_ref=slot(src, k) if ref is None else ref,
            dst_ref=slot(src, k),
            send_sem=w_send.at[way, src, k],
            recv_sem=w_recv.at[src, k],
            device_id=(target, t),
            device_id_type=MESH,
        )

    def along(src, k, ref=None):
        @pl.when(a < na - 1)
        def _():
            piece(src, k, FORE, ref).start()

        @pl.when(a > 0)
        def _():
            piece(src, k, BACK, ref).start()

    pair = f + 1 - 2 * b
    piece(f, CROSS, SIDE, own(CROSS)).start()
    for k in EARLY:
        along(f, k, own(k))
        piece(f, k, SIDE, own(k)).start()
    locals_ = [
        pltpu.make_async_copy(stream_ref, stream_all.at[t], own_sem.at[0]),
        pltpu.make_async_copy(pool_ref, pool_all.at[f], own_sem.at[1]),
        pltpu.make_async_copy(gate_ref, gate_all.at[f], own_sem.at[2]),
        pltpu.make_async_copy(up_ref, up_all.at[f], own_sem.at[3]),
        pltpu.make_async_copy(down_ref, down_all.at[f], own_sem.at[4]),
    ]
    for copy in locals_:
        copy.start()

    def arrive(src, k, way):
        piece(src, k, way).wait_recv()
        if way == FORE:

            @pl.when(a < na - 1)
            def _():
                piece(src, k, FORE).start()

        else:

            @pl.when(a > 0)
            def _():
                piece(src, k, BACK).start()

    def events(d, ks):
        for k in ks:
            for way in (FORE, BACK):
                source = a - d if way == FORE else a + d

                @pl.when((source >= 0) & (source < na))
                def _():
                    src = source * 2 + b
                    arrive(src, k, way)
                    if k == CROSS:
                        arrive(source * 2 + 1 - b, k, way)
                    else:
                        piece(src, k, SIDE).start()

    for i in range(1, fs):
        src = lax.rem(f + i, fs)
        pltpu.make_async_remote_copy(
            src_ref=pool_ref,
            dst_ref=pool_all.at[src],
            send_sem=p_send.at[src],
            recv_sem=p_recv.at[src],
            device_id=(src, t),
            device_id_type=MESH,
        ).wait_recv()
    for copy in locals_:
        copy.wait()
    _, chans, outs = pool_ref.shape
    spread_rows = one_hot(
        GROUPS * chans,
        GROUPS * chans,
        lambda r, c: c == (r % GROUPS) * chans + r // GROUPS,
    )
    spread_cols = [
        one_hot(outs, GROUPS * outs, lambda r, c, g=g: c == r * GROUPS + g)
        for g in range(GROUPS)
    ]

    def densify(s, carry):
        wide = jnp.concatenate(
            [
                jnp.dot(
                    pool_all[s, g], spread_cols[g], preferred_element_type=jnp.float32
                )
                for g in range(GROUPS)
            ],
            axis=0,
        ).astype(jnp.bfloat16)
        rows = pl.ds(pl.multiple_of(s * GROUPS * chans, GROUPS * chans), GROUPS * chans)
        dense[rows, :] = jnp.dot(
            spread_rows, wide, preferred_element_type=jnp.float32
        ).astype(jnp.bfloat16)
        return carry

    lax.fori_loop(0, fs, densify, 0)

    act_relay(0, stream_ref, stream_all)

    def factor(buf, rows):
        square = jnp.zeros((LEN, 1), jnp.float32)
        for i in range(tp):
            v = buf[i, rows, :].astype(jnp.float32)
            square = square + jnp.sum(v * v, axis=-1, keepdims=True)
        return lax.rsqrt(square / (tp * block) + epsilon)

    def pool_seq(q, carry):
        rows = pl.ds(pl.multiple_of(q * LEN, LEN), LEN)
        scale = factor(stream_all, rows)
        lane = lax.broadcasted_iota(jnp.int32, (LEN, block), 1) % GROUPS
        row = lax.broadcasted_iota(jnp.int32, (LEN, block), 0)
        extent = jnp.where(lane == 0, 2, jnp.where(lane == 1, 4, jnp.where(lane == 2, 8, 16)))
        divisor = jnp.minimum(row + 1, extent).astype(jnp.float32)
        for i in range(tp):
            v = stream_all[i, rows, :].astype(jnp.float32)
            v = v * scale * gain_mix_ref[:, i * block : (i + 1) * block]
            v = v.astype(jnp.bfloat16).astype(jnp.float32)
            running = v + delayed(v, 1)
            picked = running
            for g, amount in ((1, 2), (2, 4), (3, 8)):
                running = running + delayed(running, amount)
                picked = jnp.where(lane >= g, running, picked)
            pooled[rows, i * block : (i + 1) * block] = (picked / divisor - v).astype(
                jnp.bfloat16
            )
        return carry

    lax.fori_loop(0, seqs, pool_seq, 0)

    def mix_seq(q, carry):
        rows = pl.ds(pl.multiple_of(q * LEN, LEN), LEN)
        mixed = jnp.dot(pooled[rows, :], dense[...], preferred_element_type=jnp.float32)
        total[rows, :] = (
            stream_ref[rows, :].astype(jnp.float32) + mixed * pool_gain_ref[...]
        ).astype(jnp.bfloat16)
        return carry

    lax.fori_loop(0, seqs, mix_seq, 0)

    act_start(1, total, middle_all)
    keep = pltpu.make_async_copy(total, middle_all.at[t], own_sem.at[0])
    keep.start()
    events(1, EARLY)
    gate_sum[...] = jnp.zeros_like(gate_sum)
    value_sum[...] = jnp.zeros_like(value_sum)
    keep.wait()
    act_relay(1, total, middle_all)

    def norm_seq(q, carry):
        rows = pl.ds(pl.multiple_of(q * LEN, LEN), LEN)
        scale = factor(middle_all, rows)
        for i in range(tp):
            span = slice(i * block, (i + 1) * block)
            v = middle_all[i, rows, :].astype(jnp.float32)
            normed_ffn[rows, span] = (v * scale * gain_ffn_ref[:, span]).astype(jnp.bfloat16)
        return carry

    lax.fori_loop(0, seqs, norm_seq, 0)

    def sources(d, take):
        def one(i, carry):
            far, up = i // 2, i % 2
            dist = d - far
            source = a + (2 * up - 1) * dist
            src = source * 2 + b + far - 2 * b * far
            exists = (source >= 0) & (source < na) & (dist >= 0) & (dist < na)

            @pl.when(exists & ((dist > 0) | (up == 0)))
            def _():
                take(src, source, far)

            return carry

        lax.fori_loop(0, 4, one, 0)

    half = tokens // 2

    def project(src, source, far):
        @pl.when(far == 1)
        def _():
            for k in EARLY:
                piece(src, k, SIDE).wait_recv()

        span = pl.ds(pl.multiple_of(src * depth, depth), depth)

        def chunk(m, carry):
            rows = pl.ds(pl.multiple_of(m * half, half), half)
            left = normed_ffn[rows, span]
            gate_sum[rows, :] += jnp.dot(
                left, gate_all[src], preferred_element_type=jnp.float32
            )
            value_sum[rows, :] += jnp.dot(
                left, up_all[src], preferred_element_type=jnp.float32
            )
            return carry

        lax.fori_loop(0, 2, chunk, 0)

    def late_start():
        along(f, LATE, own(LATE))
        piece(f, LATE, SIDE, own(LATE)).start()
        along(f, CROSS, own(CROSS))
        piece(pair, CROSS, SIDE).wait_recv()
        along(pair, CROSS)

    def early_round(d, carry):
        @pl.when((d >= 1) & (d <= na - 2))
        def _():
            events(d + 1, EARLY)

        @pl.when(d == na - 2)
        def _():
            late_start()

        @pl.when(d >= na - 1)
        def _():
            events(d - na + 2, (LATE, CROSS))

        sources(d, project)
        return carry

    lax.fori_loop(0, na + 1, early_round, 0)

    def gate_seq(q, carry):
        rows = pl.ds(pl.multiple_of(q * LEN, LEN), LEN)

        def conv(sums, taps):
            v = sums[rows, :].astype(jnp.bfloat16).astype(jnp.float32)
            reach = taps.shape[0]
            running = v * taps[reach - 1 : reach, :]
            for i in range(1, reach):
                running = running + delayed(v, i) * taps[reach - 1 - i : reach - i, :]
            return running

        gate = conv(gate_sum, gate_taps_ref)
        value = conv(value_sum, up_taps_ref)
        hidden[rows, :] = (gate / (1.0 + jnp.exp(-gate)) * value).astype(jnp.bfloat16)
        return carry

    lax.fori_loop(0, seqs, gate_seq, 0)

    def part_copy(src, source, col):
        return pltpu.make_async_remote_copy(
            src_ref=part.at[src],
            dst_ref=theirs.at[t, col],
            send_sem=r_send.at[src],
            recv_sem=r_recv.at[t, col],
            device_id=(f, source),
            device_id_type=MESH,
        )

    def finish(src, source, far):
        @pl.when(far == 1)
        def _():
            piece(src, LATE, SIDE).wait_recv()

        part[src] = jnp.dot(
            hidden[...], down_all[src], preferred_element_type=jnp.float32
        ).astype(jnp.bfloat16)

        @pl.when(source != t)
        def _():
            part_copy(src, source, src % 2).start()

    def late_round(d, carry):
        @pl.when((d >= 2) & (d + 1 < na))
        def _():
            events(d + 1, (LATE,))

        @pl.when((d >= 3) & (d < na))
        def _():
            events(d, (CROSS,))

        sources(d, finish)
        return carry

    lax.fori_loop(0, na + 1, late_round, 0)

    for col in range(2):
        for i in range(1, tp):
            peer = lax.rem(t + i, tp)
            pltpu.make_async_remote_copy(
                src_ref=part.at[0],
                dst_ref=theirs.at[peer, col],
                send_sem=r_send.at[0],
                recv_sem=r_recv.at[peer, col],
                device_id=(f, peer),
                device_id_type=MESH,
            ).wait_recv()
        summed = part[2 * t + col].astype(jnp.float32)
        for i in range(1, tp):
            summed = summed + theirs[lax.rem(t + i, tp), col].astype(jnp.float32)
        out_ref[:, col * cols : (col + 1) * cols] = summed.astype(out_ref.dtype)

    for i in range(1, fs):
        pool_copy(lax.rem(f + i, fs)).wait_send()
    act_finish(0, stream_ref, stream_all)
    act_finish(1, total, middle_all)

    def drain(s, carry):
        for k in range(6):
            line, col = s // 2, s % 2
            mine = (col == b) | (k == CROSS)

            @pl.when(mine & (a < na - 1) & (line <= a))
            def _():
                piece(s, k, FORE).wait_send()

            @pl.when(mine & (a > 0) & (line >= a))
            def _():
                piece(s, k, BACK).wait_send()

            @pl.when((s == f) if k == CROSS else (col == b))
            def _():
                piece(s, k, SIDE).wait_send()

        @pl.when(s // 2 != t)
        def _():
            part_copy(s, s // 2, s % 2).wait_send()

        return carry

    lax.fori_loop(0, fs, drain, 0)


MAIN, MATE, ACROSS = 0, 1, 2


def split_kernel(
    fs,
    tp,
    stream_ref,
    gain_mix_ref,
    pool_ref,
    pool_gain_ref,
    gain_ffn_ref,
    gate_ref,
    up_ref,
    gate_taps_ref,
    up_taps_ref,
    down_ref,
    out_ref,
    gate_all,
    up_all,
    down_all,
    pool_all,
    stream_all,
    middle_all,
    pooled,
    dense,
    normed_ffn,
    gate_sum,
    value_sum,
    hidden,
    part,
    mate_part,
    y_own,
    y_part,
    z_own,
    z_part,
    total,
    w_send,
    w_recv,
    p_send,
    p_recv,
    a_send,
    a_recv,
    b_sem,
    m_send,
    m_recv,
    y_sem,
    z_sem,
    own_sem,
):
    f = lax.axis_index("fs")
    t = lax.axis_index("tp")
    a, b = f // 2, f % 2
    tokens, block = stream_ref.shape
    depth, width = gate_ref.shape
    held = gate_all.shape[2]
    other = width - held
    seqs = tokens // LEN
    cols = down_ref.shape[1]
    mate = t + 1 - 2 * (t % 2)
    across_y = lax.rem(t + 2, tp)
    h = a // 2
    has_mid = t % 2 == h
    near = a + 1 - 2 * (a % 2)
    far_in, far_out = 2 - h, 3 * (1 - h)
    inner = (a == 1) | (a == 2)
    first = jnp.where(inner, far_in, near)
    second = jnp.where(inner, far_out, far_in)
    third = jnp.where(inner, near, far_out)
    partner = lax.rem(f + fs // 2, fs)
    pair = f + 1 - 2 * b

    barrier = pltpu.get_barrier_semaphore()
    for i in range(1, fs):
        pl.semaphore_signal(
            barrier, inc=1, device_id=(lax.rem(f + i, fs), t), device_id_type=MESH
        )
    for i in range(1, tp):
        pl.semaphore_signal(
            barrier, inc=1, device_id=(f, lax.rem(t + i, tp)), device_id_type=MESH
        )
    pl.semaphore_wait(barrier, fs + tp - 2)

    def act_view(step):
        buf = stream_all if step < 2 else middle_all
        return lambda owner: buf.at[owner, pl.ds((step % 2) * tokens, tokens)]

    def act_copy(step, src, owner, target, role):
        return pltpu.make_async_remote_copy(
            src_ref=src,
            dst_ref=act_view(step)(owner),
            send_sem=a_send.at[step, role],
            recv_sem=a_recv.at[step, owner],
            device_id=(f, target),
            device_id_type=MESH,
        )

    def act_start(step, src):
        act_copy(step, src, t, across_y, 0).start()
        act_copy(step, src, t, mate, 1).start()

    def act_relay(step):
        view = act_view(step)
        act_copy(step, view(across_y), across_y, mate, 2).wait_recv()
        act_copy(step, view(across_y), across_y, mate, 2).start()
        act_copy(step, view(mate), mate, mate, 2).wait_recv()
        diagonal = lax.rem(mate + 2, tp)
        act_copy(step, view(diagonal), diagonal, mate, 2).wait_recv()

    def act_finish(step):
        view = act_view(step)
        for role in range(3):
            act_copy(step, view(t), t, mate, role).wait_send()

    def pool_copy(target, owner):
        return pltpu.make_async_remote_copy(
            src_ref=pool_ref,
            dst_ref=pool_all.at[owner],
            send_sem=p_send.at[target],
            recv_sem=p_recv.at[owner],
            device_id=(target, t),
            device_id_type=MESH,
        )

    to_partner = pltpu.make_async_remote_copy(
        src_ref=stream_ref,
        dst_ref=stream_all.at[t, pl.ds(tokens, tokens)],
        send_sem=b_sem.at[0],
        recv_sem=b_sem.at[1],
        device_id=(partner, t),
        device_id_type=MESH,
    )

    def pool_pass(owner, ref):
        return pltpu.make_async_remote_copy(
            src_ref=ref,
            dst_ref=pool_all.at[owner],
            send_sem=p_send.at[owner // 2 * 2 + 1 - b],
            recv_sem=p_recv.at[owner],
            device_id=(pair, t),
            device_id_type=MESH,
        )

    act_start(0, stream_ref)
    for i in range(2, fs, 2):
        pool_copy(lax.rem(f + i, fs), f).start()
    pool_pass(f, pool_ref).start()

    def slot(src, k):
        full = (gate_all, up_all, down_all)[k % 3]
        span = pl.ds(0, other) if k < 3 else pl.ds(other, held - other)
        if k % 3 == 2:
            return full.at[src, span]
        return full.at[src, :, span]

    def own(q, k):
        full = (gate_ref, up_ref, down_ref)[k % 3]
        if k < 3:
            span = pl.ds(pl.multiple_of(q * held, 128), other)
        else:
            span = pl.ds(other, held - other)
        if k % 3 == 2:
            return full.at[span]
        return full.at[:, span]

    def piece(src, k, way, ref=None):
        target = (pair, near * 2 + b, far_in * 2 + b)[way]
        return pltpu.make_async_remote_copy(
            src_ref=slot(src, k) if ref is None else ref,
            dst_ref=slot(src, k),
            send_sem=w_send.at[way, src, k],
            recv_sem=w_recv.at[src, k],
            device_id=(target, t),
            device_id_type=MESH,
        )

    def guarded(k, do):
        if k < 3:
            do()
        else:
            pl.when(has_mid)(do)

    def own_across(k):
        if k < 3:
            piece(f, k, ACROSS, own(1 - h, k)).start()
        else:

            @pl.when(jnp.logical_not(has_mid))
            def _():
                piece(f, k, ACROSS, own(1 - h, k)).start()

    def own_near(k):
        guarded(k, lambda: piece(f, k, MATE, own(h, k)).start())

    def own_pair(k):
        guarded(k, lambda: piece(f, k, MAIN, own(h, k)).start())

    def events(source, ks):
        src = source * 2 + b
        for k in ks:

            def one():
                piece(src, k, MAIN).wait_recv()

                @pl.when(inner & (source // 2 != h))
                def _():
                    piece(src, k, MATE).start()

                piece(src, k, MAIN).start()

            guarded(k, one)

    def arrived(src, ks):
        for k in ks:
            guarded(k, lambda: piece(src, k, MAIN).wait_recv())

    early, late = (0, 3, 1, 4), (2, 5)
    own_pair(early[0])

    def local(k):
        return pltpu.make_async_copy(own(h, k), slot(f, k), own_sem.at[k])

    for k in range(6):
        guarded(k, lambda: local(k).start())
    keep_stream = pltpu.make_async_copy(
        stream_ref, stream_all.at[t, pl.ds(0, tokens)], own_sem.at[6]
    )
    keep_pool = pltpu.make_async_copy(pool_ref, pool_all.at[f], own_sem.at[7])
    keep_stream.start()
    keep_pool.start()

    @pl.when(jnp.logical_not(has_mid))
    def _():
        gate_all[:, :, other:] = jnp.zeros((fs, depth, held - other), jnp.bfloat16)
        up_all[:, :, other:] = jnp.zeros((fs, depth, held - other), jnp.bfloat16)
        down_all[:, other:, :] = jnp.zeros((fs, held - other, cols), jnp.bfloat16)

    for i in range(2, fs, 2):
        src = lax.rem(f + i, fs)
        pool_copy(src, src).wait_recv()
        pool_pass(src, pool_all.at[src]).start()
    to_partner.start()
    for k in early:
        own_across(k)

    @pl.when(inner)
    def _():
        for k in early:
            own_near(k)

    for k in early[1:]:
        own_pair(k)
    for k in late:
        own_across(k)
    for i in range(0, fs, 2):
        src = lax.rem(pair + i, fs)
        pool_copy(src, src).wait_recv()
    keep_pool.wait()
    _, chans, outs = pool_ref.shape
    spread_rows = one_hot(
        GROUPS * chans,
        GROUPS * chans,
        lambda r, c: c == (r % GROUPS) * chans + r // GROUPS,
    )
    spread_cols = [
        one_hot(outs, GROUPS * outs, lambda r, c, g=g: c == r * GROUPS + g)
        for g in range(GROUPS)
    ]

    def densify(s, carry):
        wide = jnp.concatenate(
            [
                jnp.dot(
                    pool_all[s, g], spread_cols[g], preferred_element_type=jnp.float32
                )
                for g in range(GROUPS)
            ],
            axis=0,
        ).astype(jnp.bfloat16)
        rows = pl.ds(pl.multiple_of(s * GROUPS * chans, GROUPS * chans), GROUPS * chans)
        dense[rows, :] = jnp.dot(
            spread_rows, wide, preferred_element_type=jnp.float32
        ).astype(jnp.bfloat16)
        return carry

    lax.fori_loop(0, fs, densify, 0)
    keep_stream.wait()
    act_relay(0)

    def factor(buf, rows):
        square = jnp.zeros((LEN, 1), jnp.float32)
        for i in range(tp):
            v = buf[i, rows, :].astype(jnp.float32)
            square = square + jnp.sum(v * v, axis=-1, keepdims=True)
        return lax.rsqrt(square / (tp * block) + epsilon)

    def pool_seq(q, carry):
        rows = pl.ds(pl.multiple_of(q * LEN, LEN), LEN)
        scale = factor(stream_all, rows)
        lane = lax.broadcasted_iota(jnp.int32, (LEN, block), 1) % GROUPS
        row = lax.broadcasted_iota(jnp.int32, (LEN, block), 0)
        extent = jnp.where(lane == 0, 2, jnp.where(lane == 1, 4, jnp.where(lane == 2, 8, 16)))
        divisor = jnp.minimum(row + 1, extent).astype(jnp.float32)
        for i in range(tp):
            v = stream_all[i, rows, :].astype(jnp.float32)
            v = v * scale * gain_mix_ref[:, i * block : (i + 1) * block]
            v = v.astype(jnp.bfloat16).astype(jnp.float32)
            running = v + delayed(v, 1)
            picked = running
            for g, amount in ((1, 2), (2, 4), (3, 8)):
                running = running + delayed(running, amount)
                picked = jnp.where(lane >= g, running, picked)
            pooled[rows, i * block : (i + 1) * block] = (picked / divisor - v).astype(
                jnp.bfloat16
            )
        mixed = jnp.dot(pooled[rows, :], dense[...], preferred_element_type=jnp.float32)
        total[rows, :] = (
            stream_all[t, rows, :].astype(jnp.float32)
            + mixed * pool_gain_ref[:, pl.ds(pl.multiple_of(t * block, 128), block)]
        ).astype(jnp.bfloat16)
        return carry

    lax.fori_loop(0, seqs, pool_seq, 0)
    ours, theirs = pl.ds(0, tokens), pl.ds(tokens, tokens)
    act_start(2, total.at[ours])
    keep = [
        pltpu.make_async_copy(total.at[span], middle_all.at[t, span], own_sem.at[8 + i])
        for i, span in enumerate((ours, theirs))
    ]
    keep[0].start()

    @pl.when(jnp.logical_not(inner))
    def _():
        for k in early:
            own_near(k)

    to_partner.wait_recv()
    act_start(1, stream_all.at[t, theirs])
    events(first, early)

    @pl.when(inner)
    def _():
        events(second, early)


    act_relay(1)
    lax.fori_loop(seqs, 2 * seqs, pool_seq, 0)
    act_start(3, total.at[theirs])
    keep[1].start()
    keep[0].wait()
    act_relay(2)

    def norm(first):
        def norm_seq(q, carry):
            rows = pl.ds(pl.multiple_of(first + q * LEN, LEN), LEN)
            scale = factor(middle_all, rows)
            for i in range(tp):
                span = slice(i * block, (i + 1) * block)
                v = middle_all[i, rows, :].astype(jnp.float32)
                normed_ffn[rows, span] = (v * scale * gain_ffn_ref[:, span]).astype(
                    jnp.bfloat16
                )
            return carry

        lax.fori_loop(0, seqs, norm_seq, 0)


    @pl.when(jnp.logical_not(inner))
    def _():
        events(second, early)

    for k in late:
        own_near(k)
        own_pair(k)
    norm(0)
    keep[1].wait()
    act_relay(3)
    norm(tokens)
    events(third, early)
    for k in range(6):
        guarded(k, lambda: local(k).wait())
    arrived(pair, early)
    for source in (near, far_in, far_out):
        arrived(source * 2 + 1 - b, early)

    chunk = 2 * LEN

    def project(m, carry):
        rows = pl.ds(pl.multiple_of(m * chunk, chunk), chunk)
        left = normed_ffn[rows, :]
        for full, sums in ((gate_all, gate_sum), (up_all, value_sum)):
            sums[rows, :] = jnp.dot(
                left,
                full[...].reshape(fs * depth, held),
                preferred_element_type=jnp.float32,
            ).astype(jnp.bfloat16)
        return carry

    def gate_seq(q, carry):
        rows = pl.ds(pl.multiple_of(q * LEN, LEN), LEN)

        def conv(sums, taps_ref):
            taps = jnp.concatenate(
                [
                    taps_ref[:, pl.ds(pl.multiple_of(t * width + h * held, 128), other)],
                    taps_ref[:, pl.ds(pl.multiple_of(t * width + other, 128), held - other)],
                ],
                axis=1,
            )
            v = sums[rows, :].astype(jnp.float32)
            reach = taps.shape[0]
            running = v * taps[reach - 1 : reach, :]
            for i in range(1, reach):
                running = running + delayed(v, i) * taps[reach - 1 - i : reach - i, :]
            return running

        gate = conv(gate_sum, gate_taps_ref)
        value = conv(value_sum, up_taps_ref)
        hidden[rows, :] = (gate / (1.0 + jnp.exp(-gate)) * value).astype(jnp.bfloat16)
        return carry

    chunks = tokens // chunk
    lax.fori_loop(0, chunks, project, 0)
    events(first, late)
    lax.fori_loop(chunks, 2 * chunks, project, 0)
    events(second, late)
    lax.fori_loop(0, 2 * seqs, gate_seq, 0)

    def source_of(i):
        far = jnp.where((i == 2) | (i == 4) | (i == 5) | (i == 7), 1, 0)
        line = jnp.where(
            (i == 0) | (i == 2),
            a,
            jnp.where((i == 3) | (i == 4), first, jnp.where(i >= 6, third, second)),
        )
        return line, line * 2 + b + far - 2 * b * far, far

    def mate_copy(s):
        return pltpu.make_async_remote_copy(
            src_ref=part.at[s],
            dst_ref=mate_part.at[s],
            send_sem=m_send.at[s],
            recv_sem=m_recv.at[s],
            device_id=(f, mate),
            device_id_type=MESH,
        )

    def y_copy(col):
        return pltpu.make_async_remote_copy(
            src_ref=y_own.at[col],
            dst_ref=y_part.at[col],
            send_sem=y_sem.at[0, col],
            recv_sem=y_sem.at[1, col],
            device_id=(f, across_y),
            device_id_type=MESH,
        )

    def z_copy(col):
        return pltpu.make_async_remote_copy(
            src_ref=z_own.at[col],
            dst_ref=z_part.at[col],
            send_sem=z_sem.at[0, col],
            recv_sem=z_sem.at[1, col],
            device_id=(partner, t),
            device_id_type=MESH,
        )

    steps = 2 * fs // 2

    def finish(i, carry):
        @pl.when(i == 4)
        def _():
            events(third, late)

        @pl.when(i < steps)
        def _():
            line, s, far = source_of(i)

            @pl.when(far == 1)
            def _():
                arrived(s, late)

            part[s] = jnp.dot(
                hidden[...], down_all[s], preferred_element_type=jnp.float32
            ).astype(jnp.bfloat16)

            @pl.when(line % 2 != t % 2)
            def _():
                mate_copy(s).start()

        @pl.when((i >= 1) & (i <= steps))
        def _():
            line, s, _ = source_of(i - 1)

            @pl.when(line % 2 == t % 2)
            def _():
                mate_copy(s).wait_recv()

                @pl.when(line != t)
                def _():
                    y_own[s % 2] = (
                        part[s].astype(jnp.float32) + mate_part[s].astype(jnp.float32)
                    ).astype(jnp.bfloat16)
                    y_copy(s % 2).start()

        @pl.when(i >= 2)
        def _():
            line, s, _ = source_of(i - 2)

            @pl.when(line == t)
            def _():
                col = s % 2
                y_copy(col).wait_recv()
                z_own[col] = (
                    part[s, theirs, :].astype(jnp.float32)
                    + mate_part[s, theirs, :].astype(jnp.float32)
                    + y_part[col, theirs, :].astype(jnp.float32)
                ).astype(jnp.bfloat16)
                z_copy(col).start()

        return carry

    lax.fori_loop(0, steps + 2, finish, 0)

    for col in range(2):
        z_copy(col).wait_recv()
        mine = pl.ds(0, tokens)
        s = 2 * t + col
        out_ref[:, col * cols : (col + 1) * cols] = (
            part[s, mine, :].astype(jnp.float32)
            + mate_part[s, mine, :].astype(jnp.float32)
            + y_part[col, mine, :].astype(jnp.float32)
            + z_part[col].astype(jnp.float32)
        ).astype(out_ref.dtype)

    for i in range(2, fs, 2):
        pool_copy(lax.rem(f + i, fs), f).wait_send()
    for i in range(0, fs, 2):
        pool_pass(lax.rem(f + i, fs), pool_ref).wait_send()
    for step in range(4):
        act_finish(step)
    to_partner.wait_send()
    for col in range(2):
        y_copy(col).wait_send()
        z_copy(col).wait_send()

    for k in range(6):
        if k < 3:
            piece(f, k, ACROSS, own(1 - h, k)).wait_send()
        else:

            @pl.when(jnp.logical_not(has_mid))
            def _():
                piece(f, k, ACROSS, own(1 - h, k)).wait_send()

        def rest():
            piece(f, k, MATE).wait_send()
            for line in (a, near, far_in, far_out):
                piece(line * 2 + b, k, MAIN).wait_send()

            @pl.when(inner)
            def _():
                for line in (far_in, far_out):
                    piece(line * 2 + b, k, MATE).wait_send()

        guarded(k, rest)

    def drain(s, carry):
        @pl.when((s // 2) % 2 != t % 2)
        def _():
            mate_copy(s).wait_send()

        return carry

    lax.fori_loop(0, fs, drain, 0)


def body(
    fs,
    tp,
    stream,
    gain_mix,
    pool_weight,
    pool_gain,
    gain_ffn,
    gate_weight,
    up_weight,
    gate_taps,
    up_taps,
    down_weight,
):
    tokens, block = stream.shape
    depth, width = gate_weight.shape
    cols = down_weight.shape[1]
    channels = gain_mix.shape[0]
    t = lax.axis_index("tp")

    def mine(values, size):
        return lax.dynamic_slice_in_dim(values, t * size, size, values.ndim - 1)

    bf16, f32 = jnp.bfloat16, jnp.float32
    dma = pltpu.SemaphoreType.DMA
    split = fs == 8 and tp == 4 and width % 256 == 128 and depth % 16 == 0
    if split:
        held = (width + 128) // 2
        run = split_kernel
        scratch = [
            pltpu.VMEM((fs, depth, held), bf16),
            pltpu.VMEM((fs, depth, held), bf16),
            pltpu.VMEM((fs, held, cols), bf16),
            pltpu.VMEM((fs,) + pool_weight.shape, bf16),
            pltpu.VMEM((tp, 2 * tokens, block), bf16),
            pltpu.VMEM((tp, 2 * tokens, block), bf16),
            pltpu.VMEM((2 * tokens, channels), bf16),
            pltpu.VMEM((channels, block), bf16),
            pltpu.VMEM((2 * tokens, channels), bf16),
            pltpu.VMEM((2 * tokens, held), bf16),
            pltpu.VMEM((2 * tokens, held), bf16),
            pltpu.VMEM((2 * tokens, held), bf16),
            pltpu.VMEM((fs, 2 * tokens, cols), bf16),
            pltpu.VMEM((fs, 2 * tokens, cols), bf16),
            pltpu.VMEM((2, 2 * tokens, cols), bf16),
            pltpu.VMEM((2, 2 * tokens, cols), bf16),
            pltpu.VMEM((2, tokens, cols), bf16),
            pltpu.VMEM((2, tokens, cols), bf16),
            pltpu.VMEM((2 * tokens, block), bf16),
            dma((3, fs, 6)),
            dma((fs, 6)),
            dma((fs,)),
            dma((fs,)),
            dma((4, 3)),
            dma((4, tp)),
            dma((2,)),
            dma((fs,)),
            dma((fs,)),
            dma((2, 2)),
            dma((2, 2)),
            dma((10,)),
        ]
    else:
        run = kernel
        scratch = [
            pltpu.VMEM((fs, depth, width), bf16),
            pltpu.VMEM((fs, depth, width), bf16),
            pltpu.VMEM((fs, width, cols), bf16),
            pltpu.VMEM((fs,) + pool_weight.shape, bf16),
            pltpu.VMEM((tp, tokens, block), bf16),
            pltpu.VMEM((tp, tokens, block), bf16),
            pltpu.VMEM((tokens, channels), bf16),
            pltpu.VMEM((channels, block), bf16),
            pltpu.VMEM((tokens, channels), bf16),
            pltpu.VMEM((tokens, width), f32),
            pltpu.VMEM((tokens, width), f32),
            pltpu.VMEM((tokens, width), bf16),
            pltpu.VMEM((fs, tokens, cols), bf16),
            pltpu.VMEM((tp, 2, tokens, cols), bf16),
            pltpu.VMEM((tokens, block), bf16),
            dma((3, fs, 6)),
            dma((fs, 6)),
            dma((fs,)),
            dma((fs,)),
            dma((2, tp, 2)),
            dma((2, tp)),
            dma((fs,)),
            dma((tp, 2)),
            dma((5,)),
        ]

    def whole(values, size):
        return values if split else mine(values, size)

    return pl.pallas_call(
        functools.partial(run, fs, tp),
        out_shape=jax.ShapeDtypeStruct((tokens, block), bf16),
        in_specs=[pl.BlockSpec(memory_space=pltpu.VMEM)] * 10,
        out_specs=pl.BlockSpec(memory_space=pltpu.VMEM),
        scratch_shapes=scratch,
        compiler_params=pltpu.CompilerParams(
            collective_id=0, has_side_effects=True, vmem_limit_bytes=64 * 1024 * 1024 - 65536
        ),
    )(
        stream,
        gain_mix.reshape(1, channels),
        pool_weight,
        whole(pool_gain, block).reshape(1, -1),
        gain_ffn.reshape(1, channels),
        gate_weight,
        up_weight,
        whole(gate_taps, width),
        whole(up_taps, width),
        down_weight,
    )


def solution(mesh):
    return jax.shard_map(
        functools.partial(body, mesh.shape["fs"], mesh.shape["tp"]),
        mesh=mesh,
        in_specs=(
            P("fs", "tp"),
            P(),
            P(None, "fs", "tp"),
            P(),
            P(),
            P("fs", "tp"),
            P("fs", "tp"),
            P(),
            P(),
            P("tp", "fs"),
        ),
        out_specs=P("fs", "tp"),
        check_vma=False,
    )
```
